32 devices in a mesh: ep: 8 (over z, y), tp: 4 (over x, core).
Axes of the slice: x: 2, y: 2, z: 4, core: 2. Of those that a mesh axis runs over, the one named last changes fastest.
Arguments:
- query_rows: bfloat16 [1024, 1024], P('ep', 'tp'), may hold values from -10 to 10
- key_rows: bfloat16 [1024, 1024], P('ep', 'tp'), may hold values from -10 to 10
- value_rows: bfloat16 [1024, 1024], P('ep', 'tp'), may hold values from -6 to 6
- key_bias: bfloat16 [1024, 16], P('ep', 'tp'), may hold values from -24 to 4
- mixer_weight: bfloat16 [1024, 2048], P('tp'), may hold values from -0.1875 to 0.1875
- mixer_gain: float32 [2048], replicated, may hold values from 0.1 to 1.9
- routed_input: bfloat16 [3072, 2048], P(('ep', 'tp')), may hold values from -6 to 6
- entry_gain: float32 [2048], replicated, may hold values from 0.1 to 1.9
- expert_index: int32 [3072, 2], P(('ep', 'tp')), may hold values from 0 to 15, all different within a row; in each aligned block of 96 rows (0 to 95, 96 to 191, ...) at most 18 rows name the same one
- route_weights: float32 [3072, 2], P(('ep', 'tp')), may hold values from 0.1 to 1
- expert_gate: bfloat16 [16, 2048, 1024], P('ep', None, 'tp'), may hold values from -0.125 to 0.125
- expert_up: bfloat16 [16, 2048, 1024], P('ep', None, 'tp'), may hold values from -0.125 to 0.125
- expert_down: bfloat16 [16, 1024, 2048], P('ep', 'tp'), may hold values from -0.1875 to 0.1875
- shared_gate: bfloat16 [2048, 1024], P(None, 'tp'), may hold values from -0.125 to 0.125
- shared_up: bfloat16 [2048, 1024], P(None, 'tp'), may hold values from -0.125 to 0.125
- shared_down: bfloat16 [1024, 2048], P('tp'), may hold values from -0.1875 to 0.1875
- exit_gain: float32 [2048], replicated, may hold values from 0.1 to 1.9
Outputs:
- mixer_out: bfloat16 [1024, 2048], P(('ep', 'tp'))
- expert_out: bfloat16 [3072, 2048], P(('ep', 'tp'))
The draws below stay inside these ranges and needn't reach their ends.
Inputs may be any that keep to these rules, and one draw needn't show every extreme that they name: `expert_index`: in each aligned block of 96 rows (the rows of one device) no expert is named by more than 18 rows, a bound that some block reaches; each row names 2 different experts.
All inputs are finite; a program needn't handle non-finite values.
Results may differ from the reference program's by a relative error of at most 0.012.
Values may be sent and summed in bfloat16 or wider, within the bound.
A program may use at most 128 MiB of HBM per device.

```python
import math
import jax
import jax.numpy as jnp
import numpy as np
from jax import lax

D = 2048
HEADS = 16
HEAD_DIM = 64
FF = 1024
FF_SH = 1024
TOPK = 2
TOK_A = 128
ROWS_B = 96
TOKENS_A = 1024
TOKENS_B = 3072
EXPERTS = 16
CAP = 18
N_EP = 8
N_TP = 4


def draw_key_bias(key, part):
    random_subkeys = jax.random.split(key, 7)
    sequence_length = TOKENS_A
    head_count = HEADS
    head_draw = jax.random.uniform(random_subkeys[0], (head_count,))
    quick_heads = (head_draw < 0.5) | (head_draw <= jnp.min(head_draw))
    keep_share = jax.random.uniform(random_subkeys[1], (head_count,), minval=0.4, maxval=1.2)
    fast_reach = jax.random.uniform(random_subkeys[2], (head_count,), minval=30.0, maxval=50.0)
    noise_shift = 3.3
    slow_level = jnp.log(keep_share / sequence_length) - noise_shift
    fast_level = -jnp.log(fast_reach) - noise_shift
    base_level = jnp.where(quick_heads, fast_level, slow_level)
    shard_count = sequence_length // TOK_A
    shard_shift = jax.random.uniform(random_subkeys[3], (shard_count, head_count), minval=-0.7, maxval=0.7)
    shard_shift = jnp.repeat(shard_shift, TOK_A, axis=0)
    roughness = 0.3 * jax.random.normal(random_subkeys[4], (sequence_length, head_count))
    logarithm_bias = base_level[None, :] + shard_shift + roughness
    spike_positions = jax.random.randint(random_subkeys[5], (3,), 0, sequence_length)
    spike_rows = jnp.any(jnp.arange(sequence_length)[:, None] == spike_positions[None, :], axis=1)
    remaining_fraction = jax.random.uniform(random_subkeys[6], (sequence_length, head_count), minval=0.2, maxval=0.5)
    spike_level = jnp.log(remaining_fraction / (1.0 - remaining_fraction))
    logarithm_bias = jnp.where(spike_rows[:, None] & (~quick_heads)[None, :], spike_level, logarithm_bias)
    return logarithm_bias.astype(jnp.float32).astype(jnp.bfloat16)


def block_levels(key, dims, cuts, low, largest):
    level, own = 1.0, jax.random.fold_in(key, 6)
    for axis_at, blocks in cuts:
        heights = jnp.exp(jax.random.uniform(jax.random.fold_in(own, axis_at), (blocks,), jnp.float32, low / len(cuts), largest / len(cuts)))
        level = level * jnp.repeat(heights, dims[axis_at] // blocks).reshape([-1 if axis == axis_at else 1 for axis in range(len(dims))])
    return level


def deal_out(own_key, own, number, rows, number_of, top, reach, skew):
    ranking = jax.random.permutation(own_key, number_of)
    heavy_load, common = shares(number_of, rows * top, reach, skew, True), shares(number_of, rows * top, reach, skew, False)
    places = jnp.arange(number_of)

    def named(tallies, offset_by):
        used = int((tallies > 0).sum())
        fixed = max(1, used // 4)
        moved = fixed + (places - fixed + offset_by * (used - fixed)) % max(1, number_of - fixed)
        return jnp.zeros((number_of,), jnp.int32).at[ranking[jnp.where(places < fixed, places, moved)]].set(jnp.asarray(tallies, jnp.int32))

    tallies = jnp.where(number % 4 == 0, named(heavy_load, number // 4), named(common, number - number // 4 - 1))
    mixed = jax.random.permutation(jax.random.fold_in(own, 3), number_of)
    source_of, receiver = mixed[0:number_of // 2 * 2:2], mixed[1:number_of // 2 * 2:2]
    margin = jnp.minimum(tallies[source_of] - 1, reach - tallies[receiver]) // 2
    margin = jnp.where((source_of == ranking[0]) | (receiver == ranking[0]) | (tallies[receiver] == 0), 0, jnp.maximum(margin, 0))
    moved = jax.random.randint(jax.random.fold_in(own, 4), (number_of // 2,), 0, 1 << 20) % (margin + 1)
    tallies = tallies.at[source_of].add(-moved).at[receiver].add(moved)
    labels = jnp.searchsorted(jnp.cumsum(tallies), jnp.arange(rows * top), side="right").astype(jnp.int32)
    listing = labels.reshape(top, rows).T
    listing = listing[jax.random.permutation(jax.random.fold_in(own, 1), rows)]
    offset_by = jax.random.randint(jax.random.fold_in(own, 2), (rows, 1), 0, top)
    return jnp.take_along_axis(listing, (jnp.arange(top)[None, :] + offset_by) % top, axis=1)


def shares(count, total, bound, slope, full):
    loads = [(1 << 20) // math.isqrt(grade ** slope) + 1 for grade in range(1, count + 1)]
    largest = bound if full else min(bound, max(-(-total // count), total * loads[0] // sum(loads)))
    least = 1 if total - largest >= count - 1 else 0
    holding, surplus = [largest] + [least] * (count - 1), total - largest - least * (count - 1)
    while surplus > 0:
        movable = [i for i in range(1, count) if holding[i] < largest] or [i for i in range(1, count) if holding[i] < bound]
        whole, left = sum([loads[i] for i in movable]), surplus
        for i in movable:
            addition = min(bound - holding[i], max(1, left * loads[i] // whole), surplus)
            holding[i] = holding[i] + addition
            surplus = surplus - addition
    return np.array(holding)


def gaussian(rng, shape, deviation, bound, cuts=(), kind=jnp.bfloat16):
    array = jax.random.normal(rng, shape, jnp.float32) * deviation
    if len(cuts) > 0:
        array = block_levels(rng, shape, cuts, -0.22, 0.18) * array
    return jnp.clip(array, min=-bound, max=bound).astype(kind)


def setup_inputs(seed: int = 0) -> dict:
    seeds = jax.random.split(jax.random.key(seed), 18)
    query_rows = gaussian(seeds[0], (TOKENS_A, HEADS * HEAD_DIM), 1.6, 10.0, ((0, 8), (1, 4)))
    key_rows = gaussian(seeds[1], (TOKENS_A, HEADS * HEAD_DIM), 1.6, 10.0, ((0, 8), (1, 4)))
    value_rows = gaussian(seeds[2], (TOKENS_A, HEADS * HEAD_DIM), 1.0, 6.0, ((0, 8), (1, 4)))
    key_bias = draw_key_bias(jax.random.fold_in(seeds[17], 71), 0)
    mixer_weight = gaussian(seeds[4], (HEADS * HEAD_DIM, D), (HEADS * HEAD_DIM) ** -0.5, 0.1875, ((0, 4),))
    mixer_gain = jnp.clip(1.0 + 0.18 * jax.random.normal(seeds[5], (D,), jnp.float32), 0.1, 1.9)
    routed_input = gaussian(seeds[6], (TOKENS_B, D), 1.0, 6.0, ((0, 32),))
    entry_gain = jnp.clip(1.0 + 0.18 * jax.random.normal(seeds[7], (D,), jnp.float32), 0.1, 1.9)
    expert_index_keys = jax.random.split(jax.random.fold_in(seeds[8], 1), TOKENS_B // ROWS_B)
    expert_index_turns = jax.random.permutation(jax.random.fold_in(seeds[8], 3), TOKENS_B // ROWS_B)
    expert_index = jax.vmap(lambda own, number: deal_out(jax.random.fold_in(seeds[8], 2), own, number, ROWS_B, EXPERTS, TOPK, CAP, 2))(expert_index_keys, expert_index_turns).reshape((TOKENS_B, TOPK))
    route_weights = jnp.clip(jnp.exp(math.log(1.0) - 2.3025851 * jax.random.uniform(seeds[9], (TOKENS_B, TOPK), jnp.float32) ** block_levels(seeds[9], (TOKENS_B, TOPK), ((0, 32),), -0.2, 0.2)), 0.1, 1.0)
    expert_gate = gaussian(seeds[10], (EXPERTS, D, FF), D ** -0.5, 0.125, ((0, 8), (2, 4)))
    expert_up = gaussian(seeds[11], (EXPERTS, D, FF), D ** -0.5, 0.125, ((0, 8), (2, 4)))
    expert_down = gaussian(seeds[12], (EXPERTS, FF, D), FF ** -0.5, 0.1875, ((0, 8), (1, 4)))
    shared_gate = gaussian(seeds[13], (D, FF_SH), D ** -0.5, 0.125, ((1, 4),))
    shared_up = gaussian(seeds[14], (D, FF_SH), D ** -0.5, 0.125, ((1, 4),))
    shared_down = gaussian(seeds[15], (FF_SH, D), FF_SH ** -0.5, 0.1875, ((0, 4),))
    exit_gain = jnp.clip(1.0 + 0.18 * jax.random.normal(seeds[16], (D,), jnp.float32), 0.1, 1.9)
    return dict(query_rows=query_rows, key_rows=key_rows, value_rows=value_rows, key_bias=key_bias, mixer_weight=mixer_weight, mixer_gain=mixer_gain, routed_input=routed_input, entry_gain=entry_gain, expert_index=expert_index, route_weights=route_weights, expert_gate=expert_gate, expert_up=expert_up, expert_down=expert_down, shared_gate=shared_gate, shared_up=shared_up, shared_down=shared_down, exit_gain=exit_gain)


EPS = 1e-06

def root_norm(values, gain_row):
    return values * lax.rsqrt(lax.optimization_barrier(jnp.mean(values * values, axis=-1, keepdims=True)) + EPS) * gain_row

def key_shards():
    shards = 1
    while shards * TOK_A < 512 and N_EP % (2 * shards) == 0:
        shards = shards * 2
    return shards

def stick_breaking(query_rows, key_rows, value_rows, key_bias):
    total_rows = query_rows.shape[0]
    block_rows = key_shards() * TOK_A
    query_split = query_rows.reshape(N_EP, TOK_A, HEADS, HEAD_DIM).astype(jnp.float32)
    keys_split = key_rows.reshape(total_rows, HEADS, HEAD_DIM).astype(jnp.float32)
    values_split = value_rows.reshape(total_rows, HEADS, HEAD_DIM).astype(jnp.float32)
    bias_split = jnp.transpose(key_bias.astype(jnp.float32))
    score_scale = HEAD_DIM ** (-0.5)

    def one_shard(shard_pair):
        shard_query, shard_index = shard_pair
        query_pos = shard_index * TOK_A + jnp.arange(TOK_A, dtype=jnp.int32)
        own_block = shard_index * TOK_A // block_rows

        def backward_turn(turn_index, carried_pair):
            output, carried = carried_pair
            block_start = ((own_block - turn_index) * block_rows).astype(jnp.int32)
            block_keys = lax.dynamic_slice_in_dim(keys_split, block_start, block_rows, 0)
            block_values = lax.dynamic_slice_in_dim(values_split, block_start, block_rows, 0)
            block_bias = lax.dynamic_slice_in_dim(bias_split, block_start, block_rows, 1)
            scores = jnp.einsum('qhd,khd->hqk', shard_query, block_keys) * score_scale + block_bias[:, None, :]
            key_pos = block_start + jnp.arange(block_rows, dtype=jnp.int32)
            causal = (key_pos[None, :] < query_pos[:, None])[None]
            fail_logs = jnp.where(causal, -jax.nn.softplus(scores), 0.0)
            later_sum = lax.cumsum(fail_logs, axis=2, reverse=True) - fail_logs + carried[:, :, None]
            weights = jnp.where(causal, jnp.exp(jax.nn.log_sigmoid(scores) + later_sum), 0.0)
            weights = lax.optimization_barrier(weights.astype(jnp.bfloat16)).astype(jnp.float32)
            output = output + jnp.einsum('hqk,khd->qhd', weights, block_values)
            return (output, carried + lax.optimization_barrier(jnp.sum(fail_logs, axis=2)))
        zero_output = jnp.zeros((TOK_A, HEADS, HEAD_DIM), jnp.float32)
        zero_carried = jnp.zeros((HEADS, TOK_A), jnp.float32)
        output, unused = lax.fori_loop(0, own_block + 1, backward_turn, (zero_output, zero_carried))
        return output
    outputs = lax.map(one_shard, (query_split, jnp.arange(N_EP, dtype=jnp.int32)))
    return outputs.reshape(total_rows, HEADS * HEAD_DIM).astype(jnp.bfloat16)

def grouped_product(left_rows, right_matrix):
    part_width = left_rows.shape[1] // N_TP
    summed = jnp.zeros((left_rows.shape[0], right_matrix.shape[1]), jnp.float32)
    for part_index in range(N_TP):
        lower = part_index * part_width
        piece_sum = jnp.dot(left_rows[:, lower:lower + part_width], right_matrix[lower:lower + part_width], preferred_element_type=jnp.float32).astype(jnp.bfloat16)
        summed = summed + lax.optimization_barrier(piece_sum).astype(jnp.float32)
    return summed

def swiglu(chosen_rows, gate_weight, up_weight):
    gate_part = jnp.dot(chosen_rows, gate_weight, preferred_element_type=jnp.float32)
    up_part = jnp.dot(chosen_rows, up_weight, preferred_element_type=jnp.float32)
    return (jax.nn.silu(gate_part) * up_part).astype(jnp.bfloat16)

def routed_experts(normed, expert_index, route_weights, expert_gate, expert_up, expert_down):
    token_count = normed.shape[0]
    flat_expert = expert_index.reshape(-1).astype(jnp.int32)
    flat_token = jnp.repeat(jnp.arange(token_count, dtype=jnp.int32), TOPK)
    flat_weight = route_weights.reshape(-1)
    sort_order = jnp.argsort(flat_expert, stable=True)
    window = token_count // ROWS_B * CAP
    sorted_token = jnp.concatenate([flat_token[sort_order], jnp.zeros((window,), jnp.int32)])
    sorted_weight = jnp.concatenate([flat_weight[sort_order], jnp.zeros((window,), flat_weight.dtype)])
    counts = jax.ops.segment_sum(jnp.ones_like(flat_expert), flat_expert, EXPERTS).astype(jnp.int32)
    starts = (jnp.cumsum(counts) - counts).astype(jnp.int32)

    def one_expert(routed, expert_number):
        first_slot = starts[expert_number]
        tokens = lax.dynamic_slice_in_dim(sorted_token, first_slot, window)
        weights = lax.dynamic_slice_in_dim(sorted_weight, first_slot, window)
        live_slots = jnp.arange(window, dtype=jnp.int32) < counts[expert_number]
        chosen_rows = normed[tokens]
        hidden = swiglu(chosen_rows, expert_gate[expert_number], expert_up[expert_number])
        output = grouped_product(hidden, expert_down[expert_number]).astype(jnp.bfloat16)
        output = lax.optimization_barrier(output).astype(jnp.float32)
        return (routed.at[tokens].add(jnp.where(live_slots, weights, 0.0)[:, None] * output), None)
    routed, unused = lax.scan(one_expert, jnp.zeros((token_count, D), jnp.float32), jnp.arange(EXPERTS, dtype=jnp.int32))
    return routed

def reference(query_rows, key_rows, value_rows, key_bias, mixer_weight, mixer_gain, routed_input, entry_gain, expert_index, route_weights, expert_gate, expert_up, expert_down, shared_gate, shared_up, shared_down, exit_gain):
    attended = stick_breaking(query_rows, key_rows, value_rows, key_bias)
    mixer_sum = grouped_product(attended, mixer_weight)
    mixer_out = root_norm(mixer_sum, mixer_gain).astype(jnp.bfloat16)
    normed = root_norm(routed_input.astype(jnp.float32), entry_gain).astype(jnp.bfloat16)
    routed = routed_experts(normed, expert_index, route_weights, expert_gate, expert_up, expert_down)
    shared_hidden = swiglu(normed, shared_gate, shared_up)
    shared = grouped_product(shared_hidden, shared_down)
    expert_out = root_norm(routed + shared, exit_gain).astype(jnp.bfloat16)
    return (mixer_out, expert_out)
```

```python
import functools

import jax
import jax.numpy as jnp
from jax import lax
from jax.experimental import pallas as pl
from jax.experimental.pallas import tpu as pltpu
from jax.sharding import PartitionSpec as P

MESH = pl.DeviceIdType.MESH
EPS = 1e-06
F32 = jnp.float32
BF16 = jnp.bfloat16


class Plan:
    def __init__(self, ep_size, tp_size, head_count, query, rows, index, gate):
        self.ep = ep_size
        self.tp = tp_size
        self.lines = ep_size // 2
        self.heads = head_count
        self.shard, self.width = query.shape
        self.head_size = self.width // head_count
        self.rows, self.model = rows.shape
        self.half = self.model // 2
        self.top = index.shape[1]
        self.local = gate.shape[0]
        self.hidden = gate.shape[2]
        self.experts = self.local * ep_size
        self.capacity = 3 * self.rows * self.top // (2 * self.experts)
        self.main = self.capacity // 16 * 16
        self.tail = self.capacity - self.main
        self.block_main = self.local * self.main
        self.block_tail = self.local * self.tail
        self.picked = self.block_main + 2 * self.block_tail
        self.block = 2 * self.block_main + 2 * self.block_tail
        self.lanes = -(-self.experts // 128) * 128
        self.padded_rows = -(-self.rows // 128) * 128


def send_of(source, target, sems, slot, place):
    return pltpu.make_async_remote_copy(
        src_ref=source,
        dst_ref=target,
        send_sem=sems[0].at[slot],
        recv_sem=sems[1].at[slot],
        device_id=place,
        device_id_type=MESH,
    )


def iota(shape, axis):
    return lax.broadcasted_iota(jnp.int32, shape, axis)


def root_norm(values, gain_row):
    return values * lax.rsqrt(jnp.mean(values * values, axis=-1, keepdims=True) + EPS) * gain_row


def silu(value):
    return value / (1.0 + jnp.exp(-value))


def tail_code(plan, place):
    row = lax.rem(place, plan.block_tail)
    return row // plan.tail * plan.capacity + plan.main + lax.rem(row, plan.tail)


def picked_code(plan, place):
    if plan.main == 0:
        return tail_code(plan, place)
    code = place // plan.main * plan.capacity + lax.rem(place, plan.main)
    if plan.tail == 0:
        return code
    after = jnp.maximum(place - plan.block_main, 0)
    return jnp.where(place < plan.block_main, code, tail_code(plan, after))


def block_code(plan, place):
    bm = plan.block_main
    if bm == 0:
        return tail_code(plan, place), place // plan.block_tail
    row = lax.rem(place, bm)
    code = row // plan.main * plan.capacity + lax.rem(row, plan.main)
    side = place // bm
    if plan.tail == 0:
        return code, side
    after = jnp.maximum(place - 2 * bm, 0)
    is_tail = place >= 2 * bm
    return (
        jnp.where(is_tail, tail_code(plan, after), code),
        jnp.where(is_tail, after // plan.block_tail, side),
    )


def layer_kernel(plan, *refs):
    (
        query_ref,
        kv_ref,
        input_ref,
        entry_ref,
        exit_ref,
        mixer_gain_ref,
        index_ref,
        route_ref,
        mixer_hbm,
        gate_hbm,
        up_hbm,
        down_hbm,
        shared_gate_hbm,
        shared_up_hbm,
        shared_down_hbm,
        mixer_out,
        expert_out,
        mixer_w,
        gate_w,
        up_w,
        down_w,
        shared_gate_w,
        shared_up_w,
        shared_down_w,
        own_all,
        info,
        info_cols,
        out,
        out_pair,
        arrived,
        part,
        near_in,
        far_out,
        far_in,
        total,
        back,
        pair_out,
        pair_in,
        shared_acc,
        shared_near,
        near_shared,
        far_shared_out,
        far_shared,
        result,
        mix_part,
        near_mix,
        far_mix_out,
        far_mix,
        kv_all,
        query_heads,
        carried,
        attended,
        weight_sem,
        own_send,
        own_recv,
        info_send,
        info_recv,
        kv_line_send,
        kv_line_recv,
        kv_pair_send,
        kv_pair_recv,
        go_send,
        go_recv,
        across_send,
        across_recv,
        partner_send,
        partner_recv,
        relay_send,
        relay_recv,
        near_send,
        near_recv,
        far_send,
        far_recv,
        return_send,
        return_recv,
        small_send,
        small_recv,
    ) = refs
    ep_size, tp_size, lines = plan.ep, plan.tp, plan.lines
    rows_n, half = plan.rows, plan.half
    bm = plan.block_main
    own_ep = lax.axis_index("ep")
    own_tp = lax.axis_index("tp")
    partner_tp = own_tp + 1 - 2 * lax.rem(own_tp, 2)
    across_tp = lax.rem(own_tp + tp_size // 2, tp_size)
    diagonal_tp = lax.rem(partner_tp + tp_size // 2, tp_size)
    line = own_ep // 2
    parity = lax.rem(own_ep, 2)
    pair_ep = own_ep + 1 - 2 * parity
    to_across = (own_ep, across_tp)
    to_partner = (own_ep, partner_tp)
    to_diagonal = (own_ep, diagonal_tp)
    to_pair = (pair_ep, own_tp)
    here = (own_ep, own_tp)

    own_sems = (own_send, own_recv)
    info_sems = (info_send, info_recv)
    kv_line_sems = (kv_line_send, kv_line_recv)
    kv_pair_sems = (kv_pair_send, kv_pair_recv)
    go_sems = (go_send, go_recv)
    across_sems = (across_send, across_recv)
    partner_sems = (partner_send, partner_recv)
    relay_sems = (relay_send, relay_recv)
    near_sems = (near_send, near_recv)
    far_sems = (far_send, far_recv)
    return_sems = (return_send, return_recv)
    small_sems = (small_send, small_recv)
    PAIR_ACROSS, PAIR_BACK, NEAR_SHARED, FAR_SHARED, NEAR_MIX, FAR_MIX = range(6)

    def to_ep(slot):
        return 2 * lax.rem(line + slot // 2, lines) + lax.rem(parity + slot, 2)

    def from_ep(slot):
        return 2 * lax.rem(line - slot // 2 + lines, lines) + lax.rem(parity + slot, 2)

    def each(first, last, action):
        lax.fori_loop(first, last, lambda step, c: (action(step), c)[1], 0)

    remote_lines = lines - 1

    def slot_of(step, side):
        return 2 * (1 + lax.rem(lines // 2 - 1 + step, max(remote_lines, 1))) + side

    barrier = pltpu.get_barrier_semaphore()

    def greet(step):
        place = lax.rem(own_ep + step, ep_size)
        pl.semaphore_signal(barrier, inc=1, device_id=(place, own_tp), device_id_type=MESH)

    each(1, ep_size, greet)
    for place in (partner_tp, across_tp, diagonal_tp):
        pl.semaphore_signal(barrier, inc=1, device_id=(own_ep, place), device_id_type=MESH)

    weights = [
        pltpu.make_async_copy(source, target, weight_sem.at[number])
        for number, (source, target) in enumerate(
            [
                (shared_gate_hbm, shared_gate_w),
                (shared_up_hbm, shared_up_w),
                (shared_down_hbm, shared_down_w),
                (gate_hbm, gate_w),
                (up_hbm, up_w),
                (down_hbm, down_w),
                (mixer_hbm, mixer_w),
            ]
        )
    ]
    for copy in weights:
        copy.start()

    normed = root_norm(input_ref[...].astype(F32), entry_ref[...]).astype(BF16)
    own_all[0] = normed

    lane = iota((rows_n, plan.lanes), 1)
    named = [lane == index_ref[:, k : k + 1] for k in range(plan.top)]
    both = jnp.zeros((rows_n, plan.lanes), F32)
    for one in named:
        both = both + jnp.where(one, 1.0, 0.0)
    earlier = jnp.where(iota((rows_n, rows_n), 0) > iota((rows_n, rows_n), 1), 1.0, 0.0)
    rank = jnp.dot(earlier.astype(BF16), both.astype(BF16), preferred_element_type=F32)
    rank = rank + lane.astype(F32) * plan.capacity
    info_lane = iota((rows_n, 128), 1)
    columns = jnp.zeros((rows_n, 128), F32)
    for k, one in enumerate(named):
        code = jnp.sum(jnp.where(one, rank, 0.0), axis=1, keepdims=True)
        columns = jnp.where(info_lane == k, code, columns)
        columns = jnp.where(info_lane == plan.top + k, route_ref[:, k : k + 1], columns)
    info_cols[...] = jnp.zeros_like(info_cols)
    info_cols[0, 0:rows_n] = columns

    def turned(value):
        return jnp.transpose(value, (1, 0))

    info[0] = turned(info_cols[0])[0:8]

    def picks(codes, rel):
        hit = codes == info[rel, 0:1, 0:rows_n]
        for k in range(1, plan.top):
            hit = hit | (codes == info[rel, k : k + 1, 0:rows_n])
        return jnp.where(hit, 1.0, 0.0).astype(BF16)

    def pack(chosen, put):
        if bm:
            put(0, bm, chosen[0:bm, 0:half])
            put(bm, 2 * bm, chosen[0:bm, half:])
        if plan.block_tail:
            side = iota((2 * plan.block_tail, half), 0) // plan.block_tail
            value = jnp.where(side == 0, chosen[bm:, 0:half], chosen[bm:, half:])
            put(2 * bm, plan.block, value)

    per_block = plan.local * plan.capacity
    picked_rows = iota((ep_size * plan.picked, 1), 0)
    picked_slot = picked_rows // plan.picked
    codes = to_ep(picked_slot) * per_block + picked_code(
        plan, lax.rem(picked_rows, plan.picked)
    )
    chosen = jnp.dot(picks(codes.astype(F32), 0), normed, preferred_element_type=F32)
    for slot in range(ep_size):

        def put_out(first, last, value, slot=slot):
            out[slot, first:last] = value.astype(BF16)

        pack(chosen[slot * plan.picked : (slot + 1) * plan.picked], put_out)

    pl.semaphore_wait(barrier, ep_size - 1 + 3)

    def own_copy(source, target, number, place):
        return send_of(own_all.at[source], own_all.at[target], own_sems, number, place)

    def info_copy(target, number, place):
        return send_of(info.at[0], info.at[target], info_sems, number, place)

    def go(slot):
        return send_of(
            out.at[slot], arrived.at[slot, 0], go_sems, slot, (to_ep(slot), own_tp)
        )

    def kv_line(source, step):
        return send_of(
            source, kv_all.at[2 * step], kv_line_sems, step, (own_ep + 2, own_tp)
        )

    def kv_pair(source, step):
        return send_of(source, kv_all.at[2 * step + 1], kv_pair_sems, step, to_pair)

    own_copy(0, 1, 0, to_across).start()
    for target, place in ((1, to_across), (2, to_partner), (3, to_diagonal)):
        info_copy(target, target, place).start()
    go(1).start()

    @pl.when(line + 1 < lines)
    def kv_first():
        kv_line(kv_ref, 1).start()

    def go_line(step):
        go(slot_of(step, 0)).start()
        go(slot_of(step, 1)).start()

    each(0, remote_lines, go_line)

    @pl.when(parity == 0)
    def kv_to_pair():
        kv_pair(kv_ref, 0).start()

    own_copy(0, 2, 1, to_partner).start()

    shard, width, heads = plan.shard, plan.width, plan.heads
    head_of = iota((shard, width), 1) // plan.head_size
    queries = query_ref[...].astype(F32) * plan.head_size ** (-0.5)
    for head in range(heads):
        query_heads[head * shard : (head + 1) * shard] = jnp.where(
            head_of == head, queries, 0.0
        ).astype(BF16)
    attended[...] = jnp.zeros_like(attended)
    carried[...] = jnp.zeros_like(carried)

    def attend_block(load, own):
        keys = load(slice(0, shard), slice(0, width))
        values = load(slice(0, shard), slice(width, 2 * width))
        bias = load(slice(shard, shard + heads), slice(0, shard)).astype(F32)
        deep = (2 * shard, 2 * shard)
        row_key, column_key = lax.rem(iota(deep, 0), shard), iota(deep, 1)
        later_of = jnp.where((row_key > column_key) | (column_key >= shard), 1.0, 0.0)
        later_of = later_of.astype(BF16)
        before = iota((shard, shard), 1) < iota((shard, shard), 0)
        scores = lax.dot_general(
            query_heads[...], keys, (((1,), (1,)), ((), ())), preferred_element_type=F32
        )
        gained = attended[...]
        for head in range(heads):
            rows = slice(head * shard, (head + 1) * shard)
            score = scores[rows] + bias[head : head + 1]
            fails = -(jnp.maximum(score, 0.0) + jnp.log(1.0 + jnp.exp(-jnp.abs(score))))
            if own:
                hits = score + fails
                fails = jnp.where(before, fails, 0.0)
            else:
                hits = score + fails
            high = fails.astype(BF16)
            low = (fails - high.astype(F32)).astype(BF16)
            sums = jnp.dot(
                jnp.concatenate([high, low], axis=1), later_of, preferred_element_type=F32
            )
            taken = carried[rows]
            weights = jnp.exp(hits + sums[:, 0:shard] + taken)
            if own:
                weights = jnp.where(before, weights, 0.0)
            product = jnp.dot(weights.astype(BF16), values, preferred_element_type=F32)
            gained = gained + jnp.where(head_of == head, product, 0.0)
            carried[rows] = taken + sums[:, shard : 2 * shard]
        attended[...] = gained

    attend_block(lambda rows, cols: kv_ref[rows, cols], True)

    def attend_slot(slot):
        attend_block(lambda rows, cols: kv_all[slot, rows, cols], False)

    def kv_step(step):
        @pl.when(step <= line)
        def one():
            block = kv_all.at[2 * step]
            send_of(block, block, kv_line_sems, step, here).wait_recv()

            @pl.when(line + 1 < lines)
            def further():
                kv_line(block, step + 1).start()

            kv_pair(block, step).start()

    def attend_step(step):
        @pl.when(step <= line)
        def one():
            other = kv_all.at[2 * step + 1]
            send_of(other, other, kv_pair_sems, step, here).wait_recv()

            def turn(side, c):
                attend_slot(2 * step + lax.rem(side + 1 - parity, 2))
                return c

            lax.fori_loop(0, 2, turn, 0)

    def landed(slot):
        block = arrived.at[slot, 0]
        return send_of(block, block, go_sems, slot, here)

    def to_side(rel, slot, target, sems, place):
        return send_of(arrived.at[slot, rel], arrived.at[slot, target], sems, slot, place)

    landed(1).wait_recv()
    to_side(0, 1, 2, partner_sems, to_partner).start()

    own_copy(1, 1, 0, here).wait_recv()
    own_copy(1, 3, 2, to_partner).start()
    info_copy(1, 1, here).wait_recv()

    def choose(target_ep, rel, put):
        place = iota((plan.picked, 1), 0)
        codes = target_ep * per_block + picked_code(plan, place)
        pack(
            jnp.dot(picks(codes.astype(F32), rel), own_all[rel], preferred_element_type=F32), put
        )

    def put_pair(first, last, value):
        out_pair[first:last] = value.astype(BF16)

    choose(pair_ep, 1, put_pair)
    pair_across = send_of(out_pair, arrived.at[1, 1], small_sems, PAIR_ACROSS, to_pair)
    pair_across.start()

    @pl.when(parity == 1)
    def attend_pair():
        block = kv_all.at[1]
        send_of(block, block, kv_pair_sems, 0, here).wait_recv()
        attend_slot(1)

    def forward(step):
        for side in range(2):
            slot = slot_of(step, side)
            landed(slot).wait_recv()
            to_side(0, slot, 1, across_sems, to_across).start()
            to_side(0, slot, 2, partner_sems, to_partner).start()

    if remote_lines:
        forward(0)
        kv_step(1)

    own_copy(2, 2, 1, here).wait_recv()
    own_copy(3, 3, 2, here).wait_recv()
    for rel in (2, 3):
        info_copy(rel, rel, here).wait_recv()
    for rel in (1, 2, 3):
        info_cols[rel, :, 0:8] = turned(info[rel])
    for copy in weights[0:3]:
        copy.wait()
    shared_rows = own_all[...].reshape(tp_size * rows_n, plan.model)
    hidden = silu(jnp.dot(shared_rows, shared_gate_w[...], preferred_element_type=F32))
    hidden = hidden * jnp.dot(shared_rows, shared_up_w[...], preferred_element_type=F32)
    shared_acc[...] = jnp.dot(
        hidden.astype(BF16), shared_down_w[...], preferred_element_type=F32
    ).reshape(shared_acc.shape)

    def put_own(first, last, value, rel):
        arrived[0, rel, first:last] = value.astype(BF16)

    arrived[0, 0] = out[0]
    for rel in (1, 2, 3):
        choose(own_ep, rel, functools.partial(put_own, rel=rel))

    blocks = 2 * tp_size
    tails = blocks * plan.tail
    folded = blocks * 2 * plan.block_tail

    def tail_move(side, by_column):
        shape = (folded, plan.local * tails) if by_column else (plan.local * tails, folded)
        sorted_at = iota(shape, 1 if by_column else 0)
        folded_at = iota(shape, 0 if by_column else 1)
        expert = sorted_at // tails
        block = lax.rem(sorted_at, tails) // plan.tail
        spot = lax.rem(sorted_at, plan.tail)
        target = (
            block * 2 * plan.block_tail + side * plan.block_tail + expert * plan.tail + spot
        )
        return jnp.where(folded_at == target, 1.0, 0.0).astype(BF16)

    def experts(first):
        pair = arrived.at[pl.ds(first, 2)]
        tail_rows = None
        if plan.tail:
            folded_rows = pair[:, :, 2 * bm : plan.block].reshape(folded, half)
            tail_rows = jnp.concatenate(
                [
                    jnp.dot(tail_move(side, False), folded_rows, preferred_element_type=F32)
                    for side in range(2)
                ],
                axis=1,
            ).astype(BF16)
        tail_results = []
        for expert in range(plan.local):
            pieces = []
            if plan.main:
                at = expert * plan.main
                left = pair[:, :, at : at + plan.main]
                right = pair[:, :, bm + at : bm + at + plan.main]
                pieces.append(
                    jnp.concatenate([left, right], axis=3).reshape(
                        blocks * plan.main, plan.model
                    )
                )
            if plan.tail:
                pieces.append(tail_rows[expert * tails : (expert + 1) * tails])
            x = pieces[0] if len(pieces) == 1 else jnp.concatenate(pieces, axis=0)
            hidden = silu(jnp.dot(x, gate_w[expert], preferred_element_type=F32))
            hidden = hidden * jnp.dot(x, up_w[expert], preferred_element_type=F32)
            result_rows = jnp.dot(
                hidden.astype(BF16), down_w[expert], preferred_element_type=F32
            ).astype(BF16)
            if plan.main:
                at = expert * plan.main
                shape = (2, tp_size, plan.main, half)
                count = blocks * plan.main
                part[pl.ds(first, 2), :, at : at + plan.main] = result_rows[
                    0:count, 0:half
                ].reshape(shape)
                part[pl.ds(first, 2), :, bm + at : bm + at + plan.main] = result_rows[
                    0:count, half:
                ].reshape(shape)
            if plan.tail:
                tail_results.append(result_rows[blocks * plan.main :])
        if plan.tail:
            ends = jnp.concatenate(tail_results, axis=0)
            value = jnp.dot(
                tail_move(0, True), ends[:, 0:half], preferred_element_type=F32
            ) + jnp.dot(tail_move(1, True), ends[:, half:], preferred_element_type=F32)
            part[pl.ds(first, 2), :, 2 * bm : plan.block] = value.astype(BF16).reshape(
                2, tp_size, 2 * plan.block_tail, half
            )

    def mixed(target_ep, rel, load):
        place = iota((1, plan.block), 1)
        code, side = block_code(plan, place)
        code = (code + target_ep * per_block).astype(F32)
        weight = jnp.zeros((rows_n, plan.block), F32)
        for k in range(plan.top):
            hit = code == info_cols[rel, 0:rows_n, k : k + 1]
            at = plan.top + k
            weight = weight + jnp.where(hit, info_cols[rel, 0:rows_n, at : at + 1], 0.0)
        sums = []
        for which in range(2):
            kept = jnp.where(side == which, weight, 0.0)
            high = kept.astype(BF16)
            low = (kept - high.astype(F32)).astype(BF16)
            value = jnp.dot(
                jnp.concatenate([high, low], axis=0), load(), preferred_element_type=F32
            )
            sums.append(value[0:rows_n] + value[rows_n:])
        return jnp.concatenate(sums, axis=1)

    def near(slot):
        return send_of(
            part.at[slot, pl.ds(2, 2)], near_in.at[slot], near_sems, slot, to_partner
        )

    block = arrived.at[1, 1]
    send_of(block, block, small_sems, PAIR_ACROSS, here).wait_recv()
    to_side(1, 1, 3, relay_sems, to_partner).start()
    to_side(2, 1, 2, partner_sems, here).wait_recv()
    to_side(3, 1, 3, relay_sems, here).wait_recv()
    for copy in weights[3:6]:
        copy.wait()
    experts(0)
    near(1).start()
    for rel in range(tp_size):
        shared_acc[rel] = shared_acc[rel] + mixed(own_ep, rel, lambda rel=rel: part[0, rel])
    shared_near[...] = shared_acc[2:4].astype(BF16)
    shared_near_copy = send_of(shared_near, near_shared, small_sems, NEAR_SHARED, to_partner)
    shared_near_copy.start()
    near(1).wait_recv()
    pair_out[...] = (part[1, 0:2].astype(F32) + near_in[1].astype(F32)).astype(BF16)
    pair_back = send_of(pair_out, pair_in, small_sems, PAIR_BACK, to_pair)
    pair_back.start()

    def relay(step):
        for side in range(2):
            slot = slot_of(step, side)
            to_side(1, slot, 1, across_sems, here).wait_recv()
            to_side(1, slot, 3, relay_sems, to_partner).start()

    def ready(step):
        for side in range(2):
            slot = slot_of(step, side)
            to_side(2, slot, 2, partner_sems, here).wait_recv()
            to_side(3, slot, 3, relay_sems, here).wait_recv()

    def far(slot):
        return send_of(far_out.at[slot], far_in.at[slot], far_sems, slot, to_across)

    def send_far(step):
        for side in range(2):
            slot = slot_of(step, side)
            near(slot).wait_recv()
            far_out[slot] = (part[slot, 1].astype(F32) + near_in[slot, 1].astype(F32)).astype(
                BF16
            )
            far(slot).start()

    def give_back(slot):
        return send_of(
            total.at[slot], back.at[slot], return_sems, slot, (from_ep(slot), own_tp)
        )

    def send_total(step):
        for side in range(2):
            slot = slot_of(step, side)
            far(slot).wait_recv()
            total[slot] = (
                part[slot, 0].astype(F32)
                + near_in[slot, 0].astype(F32)
                + far_in[slot].astype(F32)
            ).astype(BF16)
            give_back(slot).start()

    def turn(step):
        @pl.when((step >= 1) & (step < remote_lines))
        def next_line():
            forward(step)
            kv_step(step + 1)

        @pl.when(step < remote_lines)
        def attend_line():
            attend_step(step + 1)

        @pl.when((step >= 1) & (step <= remote_lines))
        def compute():
            relay(step - 1)
            ready(step - 1)
            experts(slot_of(step - 1, 0))
            for side in range(2):
                near(slot_of(step - 1, side)).start()

        @pl.when(step >= 2)
        def answer():
            send_total(step - 2)

        @pl.when((step >= 1) & (step <= remote_lines))
        def reduce_far():
            send_far(step - 1)

    if remote_lines:
        each(0, remote_lines + 2, turn)

    weights[6].wait()
    rows_out = shard // tp_size
    mixer_term = jnp.dot(
        attended[...].astype(BF16), mixer_w[...], preferred_element_type=F32
    ).astype(BF16)
    for place in range(tp_size):
        high = lax.rem(place // 2 + own_tp // 2, 2)
        low = lax.rem(place + own_tp, 2)
        mix_part[high + 2 * low] = mixer_term[place * rows_out : (place + 1) * rows_out]
    mix_near_copy = send_of(
        mix_part.at[pl.ds(2, 2)], near_mix, small_sems, NEAR_MIX, to_partner
    )
    mix_near_copy.start()

    shared_near_copy.wait_recv()
    pair_back.wait_recv()
    far_shared_out[...] = (
        shared_acc[1] + near_shared[1].astype(F32) + mixed(pair_ep, 1, lambda: pair_in[1])
    ).astype(BF16)
    shared_far_copy = send_of(far_shared_out, far_shared, small_sems, FAR_SHARED, to_across)
    shared_far_copy.start()
    mix_near_copy.wait_recv()
    far_mix_out[...] = (mix_part[1].astype(F32) + near_mix[1].astype(F32)).astype(BF16)
    mix_far_copy = send_of(far_mix_out, far_mix, small_sems, FAR_MIX, to_across)
    mix_far_copy.start()
    result[...] = (
        shared_acc[0] + near_shared[0].astype(F32) + mixed(pair_ep, 0, lambda: pair_in[0])
    )

    def take_back(step):
        for side in range(2):
            slot = slot_of(step, side)
            block = back.at[slot]
            send_of(block, block, return_sems, slot, here).wait_recv()
            result[...] = result[...] + mixed(to_ep(slot), 0, lambda: back[slot])

    each(0, remote_lines, take_back)
    shared_far_copy.wait_recv()
    combined = result[...] + far_shared[...].astype(F32)
    expert_out[...] = root_norm(combined, exit_ref[...]).astype(BF16)
    mix_far_copy.wait_recv()
    mixer_sum = (
        mix_part[0].astype(F32) + near_mix[0].astype(F32) + far_mix[...].astype(F32)
    )
    mixer_out[...] = root_norm(mixer_sum, mixer_gain_ref[...]).astype(BF16)

    own_copy(0, 1, 0, to_across).wait_send()
    own_copy(0, 2, 1, to_partner).wait_send()
    own_copy(1, 3, 2, to_partner).wait_send()
    for target, place in ((1, to_across), (2, to_partner), (3, to_diagonal)):
        info_copy(target, target, place).wait_send()
    go(1).wait_send()
    to_side(0, 1, 2, partner_sems, to_partner).wait_send()
    to_side(1, 1, 3, relay_sems, to_partner).wait_send()
    near(1).wait_send()
    for copy in (
        pair_across,
        pair_back,
        shared_near_copy,
        shared_far_copy,
        mix_near_copy,
        mix_far_copy,
    ):
        copy.wait_send()

    def finish(slot):
        go(slot).wait_send()
        to_side(0, slot, 1, across_sems, to_across).wait_send()
        to_side(0, slot, 2, partner_sems, to_partner).wait_send()
        to_side(1, slot, 3, relay_sems, to_partner).wait_send()
        near(slot).wait_send()
        far(slot).wait_send()
        give_back(slot).wait_send()

    each(2, ep_size, finish)

    def finish_kv(step):
        @pl.when((step <= line) & (line + 1 < lines))
        def sent_on():
            kv_line(kv_all.at[2 * step], step + 1).wait_send()

        @pl.when((step <= line) & (step >= 1))
        def sent_over():
            kv_pair(kv_all.at[2 * step], step).wait_send()

    each(0, lines, finish_kv)

    @pl.when(parity == 0)
    def sent_pair():
        kv_pair(kv_ref, 0).wait_send()


def on_device(
    query_rows,
    key_rows,
    value_rows,
    key_bias,
    mixer_weight,
    mixer_gain,
    routed_input,
    entry_gain,
    expert_index,
    route_weights,
    expert_gate,
    expert_up,
    expert_down,
    shared_gate,
    shared_up,
    shared_down,
    exit_gain,
):
    ep_size = lax.axis_size("ep")
    tp_size = lax.axis_size("tp")
    plan = Plan(
        ep_size, tp_size, key_bias.shape[1], query_rows, routed_input, expert_index, expert_gate
    )
    shard, width, model, rows = plan.shard, plan.width, plan.model, plan.rows
    bias_rows = -(-plan.heads // 16) * 16
    bias_block = jnp.pad(
        jnp.transpose(key_bias), ((0, bias_rows - plan.heads), (0, 2 * width - shard))
    )
    kv_block = jnp.concatenate(
        [jnp.concatenate([key_rows, value_rows], axis=1), bias_block], axis=0
    )
    small = [
        query_rows,
        kv_block,
        routed_input,
        entry_gain.reshape(1, model),
        exit_gain.reshape(1, model),
        mixer_gain.reshape(1, model),
        expert_index,
        route_weights,
    ]
    large = [
        mixer_weight,
        expert_gate,
        expert_up,
        expert_down,
        shared_gate,
        shared_up,
        shared_down,
    ]
    vmem = pl.BlockSpec(memory_space=pltpu.VMEM)
    block = (plan.block, plan.half)
    mix = (shard // tp_size, model)

    def buffer(*shape, kind=BF16):
        return pltpu.VMEM(shape, kind)

    scratch = [pltpu.VMEM(value.shape, value.dtype) for value in large]
    scratch += [
        buffer(tp_size, rows, model),
        buffer(tp_size, 8, plan.padded_rows, kind=F32),
        buffer(tp_size, plan.padded_rows, 128, kind=F32),
        buffer(ep_size, *block),
        buffer(*block),
        buffer(ep_size, tp_size, *block),
        buffer(ep_size, tp_size, *block),
        buffer(ep_size, 2, *block),
        buffer(ep_size, *block),
        buffer(ep_size, *block),
        buffer(ep_size, *block),
        buffer(ep_size, *block),
        buffer(2, *block),
        buffer(2, *block),
        buffer(tp_size, rows, model, kind=F32),
        buffer(2, rows, model),
        buffer(2, rows, model),
        buffer(rows, model),
        buffer(rows, model),
        buffer(rows, model, kind=F32),
        buffer(tp_size, *mix),
        buffer(2, *mix),
        buffer(*mix),
        buffer(*mix),
        buffer(ep_size, *kv_block.shape),
        buffer(plan.heads * shard, width),
        buffer(plan.heads * shard, shard, kind=F32),
        buffer(shard, width, kind=F32),
    ]
    sem = pltpu.SemaphoreType.DMA
    scratch += [sem((len(large),))]
    for count in (4, 4, ep_size, ep_size, ep_size, ep_size, ep_size, ep_size, ep_size, ep_size, ep_size, 6):
        scratch += [sem((count,)), sem((count,))]
    mixer_out, expert_out = pl.pallas_call(
        functools.partial(layer_kernel, plan),
        out_shape=(
            jax.ShapeDtypeStruct(mix, BF16),
            jax.ShapeDtypeStruct((rows, model), BF16),
        ),
        in_specs=[vmem] * len(small) + [pl.BlockSpec(memory_space=pl.ANY)] * len(large),
        out_specs=(vmem, vmem),
        scratch_shapes=scratch,
        compiler_params=pltpu.CompilerParams(
            collective_id=0, has_side_effects=True, vmem_limit_bytes=62 * 1024 * 1024
        ),
        name="whole_layer",
    )(*small, *large)
    return (mixer_out, expert_out)


def solution(mesh):
    in_specs = (
        P("ep", "tp"),
        P("ep", "tp"),
        P("ep", "tp"),
        P("ep", "tp"),
        P("tp", None),
        P(),
        P(("ep", "tp"), None),
        P(),
        P(("ep", "tp"), None),
        P(("ep", "tp"), None),
        P("ep", None, "tp"),
        P("ep", None, "tp"),
        P("ep", "tp", None),
        P(None, "tp"),
        P(None, "tp"),
        P("tp", None),
        P(),
    )
    out_specs = (P(("ep", "tp"), None), P(("ep", "tp"), None))
    return jax.shard_map(
        on_device, mesh=mesh, in_specs=in_specs, out_specs=out_specs, check_vma=False
    )
```

```python
import functools

import jax
import jax.numpy as jnp
from jax import lax
from jax.experimental import pallas as pl
from jax.experimental.pallas import tpu as pltpu
from jax.sharding import PartitionSpec as P

MESH = pl.DeviceIdType.MESH
EPS = 1e-06
F32 = jnp.float32
BF16 = jnp.bfloat16


class Plan:
    def __init__(self, ep_size, tp_size, head_count, query, rows, index, gate):
        self.ep = ep_size
        self.tp = tp_size
        self.lines = ep_size // 2
        self.heads = head_count
        self.shard, self.width = query.shape
        self.head_size = self.width // head_count
        self.rows, self.model = rows.shape
        self.half = self.model // 2
        self.top = index.shape[1]
        self.local = gate.shape[0]
        self.hidden = gate.shape[2]
        self.experts = self.local * ep_size
        self.capacity = 3 * self.rows * self.top // (2 * self.experts)
        self.main = self.capacity // 16 * 16
        self.tail = self.capacity - self.main
        self.block_main = self.local * self.main
        self.block_tail = self.local * self.tail
        self.picked = self.block_main + 2 * self.block_tail
        self.block = 2 * self.block_main + 2 * self.block_tail
        self.named = -(-self.experts // 16) * 16
        self.padded_rows = -(-self.rows // 128) * 128


def send_of(source, target, sems, slot, place):
    return pltpu.make_async_remote_copy(
        src_ref=source,
        dst_ref=target,
        send_sem=sems[0].at[slot],
        recv_sem=sems[1].at[slot],
        device_id=place,
        device_id_type=MESH,
    )


def got(name, copy):
    with jax.named_scope(name):
        copy.wait_recv()


def timed(name, action, *args):
    with jax.named_scope(name):
        return action(*args)


def iota(shape, axis):
    return lax.broadcasted_iota(jnp.int32, shape, axis)


def root_norm(values, gain_row):
    return values * lax.rsqrt(jnp.mean(values * values, axis=-1, keepdims=True) + EPS) * gain_row


def silu(value):
    return value / (1.0 + jnp.exp(-value))


def tail_code(plan, place):
    row = lax.rem(place, plan.block_tail)
    return row // plan.tail * plan.capacity + plan.main + lax.rem(row, plan.tail)


def picked_code(plan, place):
    if plan.main == 0:
        return tail_code(plan, place)
    code = place // plan.main * plan.capacity + lax.rem(place, plan.main)
    if plan.tail == 0:
        return code
    after = jnp.maximum(place - plan.block_main, 0)
    return jnp.where(place < plan.block_main, code, tail_code(plan, after))


def block_code(plan, place):
    bm = plan.block_main
    if bm == 0:
        return tail_code(plan, place), place // plan.block_tail
    row = lax.rem(place, bm)
    code = row // plan.main * plan.capacity + lax.rem(row, plan.main)
    side = place // bm
    if plan.tail == 0:
        return code, side
    after = jnp.maximum(place - 2 * bm, 0)
    is_tail = place >= 2 * bm
    return (
        jnp.where(is_tail, tail_code(plan, after), code),
        jnp.where(is_tail, after // plan.block_tail, side),
    )


def layer_kernel(plan, *refs):
    (
        query_ref,
        key_ref,
        value_ref,
        bias_ref,
        input_ref,
        entry_ref,
        index_ref,
        route_ref,
        mixer_hbm,
        gate_hbm,
        up_hbm,
        down_hbm,
        shared_gate_hbm,
        shared_up_hbm,
        shared_down_hbm,
        mixer_out,
        expert_out,
        mixer_w,
        gate_w,
        up_w,
        down_w,
        shared_gate_w,
        shared_up_w,
        shared_down_w,
        own_all,
        info,
        info_cols,
        out,
        out_pair,
        arrived,
        part,
        near_in,
        far_out,
        far_in,
        total,
        back,
        pair_out,
        pair_in,
        shared_acc,
        shared_near,
        near_shared,
        far_shared_out,
        far_shared,
        result,
        mix_part,
        near_mix,
        far_mix_out,
        far_mix,
        kv_ref,
        kv_all,
        query_heads,
        carried,
        attended,
        weight_sem,
        own_send,
        own_recv,
        info_send,
        info_recv,
        kv_line_send,
        kv_line_recv,
        kv_pair_send,
        kv_pair_recv,
        go_send,
        go_recv,
        across_send,
        across_recv,
        partner_send,
        partner_recv,
        relay_send,
        relay_recv,
        near_send,
        near_recv,
        far_send,
        far_recv,
        return_send,
        return_recv,
        small_send,
        small_recv,
    ) = refs
    ep_size, tp_size, lines = plan.ep, plan.tp, plan.lines
    rows_n, half = plan.rows, plan.half
    bm = plan.block_main
    own_ep = lax.axis_index("ep")
    own_tp = lax.axis_index("tp")
    partner_tp = own_tp + 1 - 2 * lax.rem(own_tp, 2)
    across_tp = lax.rem(own_tp + tp_size // 2, tp_size)
    diagonal_tp = lax.rem(partner_tp + tp_size // 2, tp_size)
    line = own_ep // 2
    parity = lax.rem(own_ep, 2)
    pair_ep = own_ep + 1 - 2 * parity
    to_across = (own_ep, across_tp)
    to_partner = (own_ep, partner_tp)
    to_diagonal = (own_ep, diagonal_tp)
    to_pair = (pair_ep, own_tp)
    here = (own_ep, own_tp)

    own_sems = (own_send, own_recv)
    info_sems = (info_send, info_recv)
    kv_line_sems = (kv_line_send, kv_line_recv)
    kv_pair_sems = (kv_pair_send, kv_pair_recv)
    go_sems = (go_send, go_recv)
    across_sems = (across_send, across_recv)
    partner_sems = (partner_send, partner_recv)
    relay_sems = (relay_send, relay_recv)
    near_sems = (near_send, near_recv)
    far_sems = (far_send, far_recv)
    return_sems = (return_send, return_recv)
    small_sems = (small_send, small_recv)
    PAIR_ACROSS, PAIR_BACK, NEAR_SHARED, FAR_SHARED, NEAR_MIX, FAR_MIX = range(6)

    def to_ep(slot):
        return 2 * lax.rem(line + slot // 2, lines) + lax.rem(parity + slot, 2)

    def from_ep(slot):
        return 2 * lax.rem(line - slot // 2 + lines, lines) + lax.rem(parity + slot, 2)

    def each(first, last, action):
        lax.fori_loop(first, last, lambda step, c: (action(step), c)[1], 0)

    remote_lines = lines - 1

    def other_line(step):
        middle = lines // 2
        inner = jnp.minimum(line, lines - 1 - line)
        index = jnp.where(step <= middle + inner - 1, step - 1, step)
        around = index < 2 * inner
        distance = jnp.where(around, index // 2 + 1, index - inner + 1)
        to_end = jnp.where(around, lax.rem(index, 2), 1)
        upward = (2 * line < lines) == (to_end == 1)
        near_line = jnp.where(upward, line + distance, line - distance)
        return jnp.where(step == 0, lax.rem(line + middle, lines), near_line)

    def slot_of(step, side):
        return 2 * lax.rem(line - other_line(step) + lines, lines) + side

    def slot_to(step, side):
        return 2 * lax.rem(other_line(step) - line + lines, lines) + side

    barrier = pltpu.get_barrier_semaphore()

    def greet(step):
        place = lax.rem(own_ep + step, ep_size)
        pl.semaphore_signal(barrier, inc=1, device_id=(place, own_tp), device_id_type=MESH)

    each(1, ep_size, greet)
    for place in (partner_tp, across_tp, diagonal_tp):
        pl.semaphore_signal(barrier, inc=1, device_id=(own_ep, place), device_id_type=MESH)

    weights = [
        pltpu.make_async_copy(source, target, weight_sem.at[number])
        for number, (source, target) in enumerate(
            [
                (shared_gate_hbm, shared_gate_w),
                (shared_up_hbm, shared_up_w),
                (shared_down_hbm, shared_down_w),
                (gate_hbm, gate_w),
                (up_hbm, up_w),
                (down_hbm, down_w),
                (mixer_hbm, mixer_w),
            ]
        )
    ]
    for copy in weights:
        copy.start()

    normed = root_norm(input_ref[...].astype(F32), entry_ref[...]).astype(BF16)
    own_all[0] = normed

    with jax.named_scope("wait_barrier"):
        pl.semaphore_wait(barrier, ep_size - 1 + 3)

    def own_copy(source, target, number, place):
        return send_of(own_all.at[source], own_all.at[target], own_sems, number, place)

    own_copy(0, 1, 0, to_across).start()
    own_copy(0, 2, 1, to_partner).start()

    expert_at = iota((plan.named, rows_n), 0)
    named = [expert_at == index_ref[k : k + 1] for k in range(plan.top)]
    both = jnp.zeros((plan.named, rows_n), F32)
    for one in named:
        both = both + jnp.where(one, 1.0, 0.0)
    earlier = jnp.where(iota((rows_n, rows_n), 0) < iota((rows_n, rows_n), 1), 1.0, 0.0)
    rank = jnp.dot(both.astype(BF16), earlier.astype(BF16), preferred_element_type=F32)
    rank = rank + expert_at.astype(F32) * plan.capacity
    info[0] = jnp.zeros_like(info[0])
    for k, one in enumerate(named):
        code = jnp.sum(jnp.where(one, rank, 0.0), axis=0, keepdims=True)
        info[0, k : k + 1, 0:rows_n] = code
        info[0, plan.top + k : plan.top + k + 1, 0:rows_n] = route_ref[k : k + 1]

    def turned(value):
        return jnp.transpose(value, (1, 0))

    def picks(codes, rel):
        hit = codes == info[rel, 0:1, 0:rows_n]
        for k in range(1, plan.top):
            hit = hit | (codes == info[rel, k : k + 1, 0:rows_n])
        return jnp.where(hit, 1.0, 0.0).astype(BF16)

    def pack(chosen, put):
        if bm:
            put(0, bm, chosen[0:bm, 0:half])
            put(bm, 2 * bm, chosen[0:bm, half:])
        if plan.block_tail:
            side = iota((2 * plan.block_tail, half), 0) // plan.block_tail
            value = jnp.where(side == 0, chosen[bm:, 0:half], chosen[bm:, half:])
            put(2 * bm, plan.block, value)

    per_block = plan.local * plan.capacity
    picked_rows = iota((ep_size * plan.picked, 1), 0)
    picked_slot = picked_rows // plan.picked
    codes = to_ep(picked_slot) * per_block + picked_code(
        plan, lax.rem(picked_rows, plan.picked)
    )
    chosen = jnp.dot(picks(codes.astype(F32), 0), normed, preferred_element_type=F32)
    for slot in range(ep_size):

        def put_out(first, last, value, slot=slot):
            out[slot, first:last] = value.astype(BF16)

        pack(chosen[slot * plan.picked : (slot + 1) * plan.picked], put_out)

    shard, width, heads = plan.shard, plan.width, plan.heads
    kv_ref[0:shard, 0:width] = key_ref[...]
    kv_ref[0:shard, width:] = value_ref[...]
    kv_ref[shard:] = jnp.zeros((kv_ref.shape[0] - shard, 2 * width), BF16)
    kv_ref[shard : shard + heads, 0:shard] = bias_ref[...]

    def info_copy(target, number, place):
        return send_of(info.at[0], info.at[target], info_sems, number, place)

    def go(slot):
        return send_of(
            out.at[slot], arrived.at[slot, 0], go_sems, slot, (to_ep(slot), own_tp)
        )

    def kv_line(source, step):
        return send_of(
            source, kv_all.at[2 * step], kv_line_sems, step, (own_ep + 2, own_tp)
        )

    def kv_pair(source, step):
        return send_of(source, kv_all.at[2 * step + 1], kv_pair_sems, step, to_pair)

    for target, place in ((1, to_across), (2, to_partner), (3, to_diagonal)):
        info_copy(target, target, place).start()
    go(1).start()

    def go_line(step):
        go(slot_to(step, 0)).start()
        go(slot_to(step, 1)).start()

    early = max(remote_lines - 1, 0)
    each(0, early, go_line)

    @pl.when(line + 1 < lines)
    def kv_first():
        kv_line(kv_ref, 1).start()

    each(early, remote_lines, go_line)

    @pl.when(parity == 0)
    def kv_to_pair():
        kv_pair(kv_ref, 0).start()

    head_of = iota((shard, width), 1) // plan.head_size
    queries = query_ref[...].astype(F32) * plan.head_size ** (-0.5)
    for head in range(heads):
        query_heads[head * shard : (head + 1) * shard] = jnp.where(
            head_of == head, queries, 0.0
        ).astype(BF16)
    attended[...] = jnp.zeros_like(attended)
    carried[...] = jnp.zeros_like(carried)

    def attend_block(load, own):
        keys = load(slice(0, shard), slice(0, width))
        values = load(slice(0, shard), slice(width, 2 * width))
        bias = load(slice(shard, shard + heads), slice(0, shard)).astype(F32)
        deep = (2 * shard, 2 * shard)
        row_key, column_key = lax.rem(iota(deep, 0), shard), iota(deep, 1)
        later_of = jnp.where((row_key > column_key) | (column_key >= shard), 1.0, 0.0)
        later_of = later_of.astype(BF16)
        before = iota((shard, shard), 1) < iota((shard, shard), 0)
        scores = lax.dot_general(
            query_heads[...], keys, (((1,), (1,)), ((), ())), preferred_element_type=F32
        )
        gained = attended[...]
        for head in range(heads):
            rows = slice(head * shard, (head + 1) * shard)
            score = scores[rows] + bias[head : head + 1]
            fails = -(jnp.maximum(score, 0.0) + jnp.log(1.0 + jnp.exp(-jnp.abs(score))))
            if own:
                hits = score + fails
                fails = jnp.where(before, fails, 0.0)
            else:
                hits = score + fails
            high = fails.astype(BF16)
            low = (fails - high.astype(F32)).astype(BF16)
            sums = jnp.dot(
                jnp.concatenate([high, low], axis=1), later_of, preferred_element_type=F32
            )
            taken = carried[rows]
            weights = jnp.exp(hits + sums[:, 0:shard] + taken)
            if own:
                weights = jnp.where(before, weights, 0.0)
            product = jnp.dot(weights.astype(BF16), values, preferred_element_type=F32)
            gained = gained + jnp.where(head_of == head, product, 0.0)
            carried[rows] = taken + sums[:, shard : 2 * shard]
        attended[...] = gained

    timed("attend_own", attend_block, lambda rows, cols: kv_ref[rows, cols], True)

    def attend_slot(slot):
        attend_block(lambda rows, cols: kv_all[slot, rows, cols], False)

    def kv_step(step):
        @pl.when(step <= line)
        def one():
            block = kv_all.at[2 * step]
            got("wait_kv_line", send_of(block, block, kv_line_sems, step, here))

            @pl.when(line + 1 < lines)
            def further():
                kv_line(block, step + 1).start()

            kv_pair(block, step).start()

    def attend_step(step):
        @pl.when(step <= line)
        def one():
            other = kv_all.at[2 * step + 1]
            got("wait_kv_pair", send_of(other, other, kv_pair_sems, step, here))

            def turn(side, c):
                timed("attend", attend_slot, 2 * step + lax.rem(side + 1 - parity, 2))
                return c

            lax.fori_loop(0, 2, turn, 0)

    def landed(slot):
        block = arrived.at[slot, 0]
        return send_of(block, block, go_sems, slot, here)

    def to_side(rel, slot, target, sems, place):
        return send_of(arrived.at[slot, rel], arrived.at[slot, target], sems, slot, place)

    got("wait_pair", landed(1))
    to_side(0, 1, 2, partner_sems, to_partner).start()

    got("wait_own_across", own_copy(1, 1, 0, here))
    own_copy(1, 3, 2, to_partner).start()
    info_copy(1, 1, here).wait_recv()

    def choose(target_ep, rel, put):
        place = iota((plan.picked, 1), 0)
        codes = target_ep * per_block + picked_code(plan, place)
        pack(
            jnp.dot(picks(codes.astype(F32), rel), own_all[rel], preferred_element_type=F32), put
        )

    def put_pair(first, last, value):
        out_pair[first:last] = value.astype(BF16)

    choose(pair_ep, 1, put_pair)
    pair_across = send_of(out_pair, arrived.at[1, 1], small_sems, PAIR_ACROSS, to_pair)
    pair_across.start()

    def forward_side(step, side):
        slot = slot_of(step, side)
        got("wait_landed", landed(slot))
        to_side(0, slot, 1, across_sems, to_across).start()
        to_side(0, slot, 2, partner_sems, to_partner).start()

    def forward(step):
        for side in range(2):
            forward_side(step, side)

    if remote_lines:
        forward_side(0, 0)

    got("wait_own_partner", own_copy(2, 2, 1, here))
    got("wait_own_diag", own_copy(3, 3, 2, here))
    for rel in (2, 3):
        info_copy(rel, rel, here).wait_recv()
    for rel in range(tp_size):
        info_cols[rel, :, 0:8] = turned(info[rel])
    for copy in weights[0:3]:
        copy.wait()

    def shared_expert():
        shared_rows = own_all[...].reshape(tp_size * rows_n, plan.model)
        hidden = silu(jnp.dot(shared_rows, shared_gate_w[...], preferred_element_type=F32))
        hidden = hidden * jnp.dot(shared_rows, shared_up_w[...], preferred_element_type=F32)
        shared_acc[...] = jnp.dot(
            hidden.astype(BF16), shared_down_w[...], preferred_element_type=F32
        ).reshape(shared_acc.shape)

    timed("shared", shared_expert)
    if remote_lines:
        forward_side(0, 1)

    def put_own(first, last, value, rel):
        arrived[0, rel, first:last] = value.astype(BF16)

    def choose_own():
        arrived[0, 0] = out[0]
        for rel in (1, 2, 3):
            choose(own_ep, rel, functools.partial(put_own, rel=rel))

    timed("choose_own", choose_own)

    blocks = 2 * tp_size
    tails = blocks * plan.tail
    folded = blocks * 2 * plan.block_tail

    def tail_move(side, by_column):
        shape = (folded, plan.local * tails) if by_column else (plan.local * tails, folded)
        sorted_at = iota(shape, 1 if by_column else 0)
        folded_at = iota(shape, 0 if by_column else 1)
        expert = sorted_at // tails
        block = lax.rem(sorted_at, tails) // plan.tail
        spot = lax.rem(sorted_at, plan.tail)
        target = (
            block * 2 * plan.block_tail + side * plan.block_tail + expert * plan.tail + spot
        )
        return jnp.where(folded_at == target, 1.0, 0.0).astype(BF16)

    def experts(first):
        pair = arrived.at[pl.ds(first, 2)]
        tail_rows = None
        if plan.tail:
            folded_rows = pair[:, :, 2 * bm : plan.block].reshape(folded, half)
            tail_rows = jnp.concatenate(
                [
                    jnp.dot(tail_move(side, False), folded_rows, preferred_element_type=F32)
                    for side in range(2)
                ],
                axis=1,
            ).astype(BF16)
        tail_results = []
        for expert in range(plan.local):
            pieces = []
            if plan.main:
                at = expert * plan.main
                left = pair[:, :, at : at + plan.main]
                right = pair[:, :, bm + at : bm + at + plan.main]
                pieces.append(
                    jnp.concatenate([left, right], axis=3).reshape(
                        blocks * plan.main, plan.model
                    )
                )
            if plan.tail:
                pieces.append(tail_rows[expert * tails : (expert + 1) * tails])
            x = pieces[0] if len(pieces) == 1 else jnp.concatenate(pieces, axis=0)
            hidden = silu(jnp.dot(x, gate_w[expert], preferred_element_type=F32))
            hidden = hidden * jnp.dot(x, up_w[expert], preferred_element_type=F32)
            result_rows = jnp.dot(
                hidden.astype(BF16), down_w[expert], preferred_element_type=F32
            ).astype(BF16)
            if plan.main:
                at = expert * plan.main
                shape = (2, tp_size, plan.main, half)
                count = blocks * plan.main
                part[pl.ds(first, 2), :, at : at + plan.main] = result_rows[
                    0:count, 0:half
                ].reshape(shape)
                part[pl.ds(first, 2), :, bm + at : bm + at + plan.main] = result_rows[
                    0:count, half:
                ].reshape(shape)
            if plan.tail:
                tail_results.append(result_rows[blocks * plan.main :])
        if plan.tail:
            ends = jnp.concatenate(tail_results, axis=0)
            value = jnp.dot(
                tail_move(0, True), ends[:, 0:half], preferred_element_type=F32
            ) + jnp.dot(tail_move(1, True), ends[:, half:], preferred_element_type=F32)
            part[pl.ds(first, 2), :, 2 * bm : plan.block] = value.astype(BF16).reshape(
                2, tp_size, 2 * plan.block_tail, half
            )

    def mixed(target_ep, rel, load):
        place = iota((1, plan.block), 1)
        code, side = block_code(plan, place)
        code = (code + target_ep * per_block).astype(F32)
        weight = jnp.zeros((rows_n, plan.block), F32)
        for k in range(plan.top):
            hit = code == info_cols[rel, 0:rows_n, k : k + 1]
            at = plan.top + k
            weight = weight + jnp.where(hit, info_cols[rel, 0:rows_n, at : at + 1], 0.0)
        sums = []
        for which in range(2):
            kept = jnp.where(side == which, weight, 0.0)
            high = kept.astype(BF16)
            low = (kept - high.astype(F32)).astype(BF16)
            value = jnp.dot(
                jnp.concatenate([high, low], axis=0), load(), preferred_element_type=F32
            )
            sums.append(value[0:rows_n] + value[rows_n:])
        return jnp.concatenate(sums, axis=1)

    def near(slot):
        return send_of(
            part.at[slot, pl.ds(2, 2)], near_in.at[slot], near_sems, slot, to_partner
        )

    block = arrived.at[1, 1]
    got("wait_pair_across", send_of(block, block, small_sems, PAIR_ACROSS, here))
    to_side(1, 1, 3, relay_sems, to_partner).start()
    got("wait_pair_p", to_side(2, 1, 2, partner_sems, here))
    got("wait_pair_r", to_side(3, 1, 3, relay_sems, here))
    for copy in weights[3:6]:
        copy.wait()
    timed("experts_own", experts, 0)
    near(1).start()
    if remote_lines > 1:
        forward(1)

    def fold_own():
        for rel in range(tp_size):
            shared_acc[rel] = shared_acc[rel] + mixed(own_ep, rel, lambda rel=rel: part[0, rel])

    timed("fold_own", fold_own)
    shared_near[...] = shared_acc[2:4].astype(BF16)
    shared_near_copy = send_of(shared_near, near_shared, small_sems, NEAR_SHARED, to_partner)
    shared_near_copy.start()
    got("wait_near1", near(1))
    pair_out[...] = (part[1, 0:2].astype(F32) + near_in[1].astype(F32)).astype(BF16)
    pair_back = send_of(pair_out, pair_in, small_sems, PAIR_BACK, to_pair)
    pair_back.start()

    @pl.when(parity == 1)
    def attend_pair():
        block = kv_all.at[1]
        got("wait_kv_pair", send_of(block, block, kv_pair_sems, 0, here))
        timed("attend", attend_slot, 1)

    def relay(step):
        for side in range(2):
            slot = slot_of(step, side)
            got("wait_across", to_side(1, slot, 1, across_sems, here))
            to_side(1, slot, 3, relay_sems, to_partner).start()

    def ready(step):
        for side in range(2):
            slot = slot_of(step, side)
            got("wait_partner", to_side(2, slot, 2, partner_sems, here))
            got("wait_relay", to_side(3, slot, 3, relay_sems, here))

    def far(slot):
        return send_of(far_out.at[slot], far_in.at[slot], far_sems, slot, to_across)

    def send_far(step):
        for side in range(2):
            slot = slot_of(step, side)
            got("wait_near", near(slot))
            far_out[slot] = (part[slot, 1].astype(F32) + near_in[slot, 1].astype(F32)).astype(
                BF16
            )
            far(slot).start()

    def give_back(slot):
        return send_of(
            total.at[slot], back.at[slot], return_sems, slot, (from_ep(slot), own_tp)
        )

    def send_total(step):
        for side in range(2):
            slot = slot_of(step, side)
            got("wait_far", far(slot))
            total[slot] = (
                part[slot, 0].astype(F32)
                + near_in[slot, 0].astype(F32)
                + far_in[slot].astype(F32)
            ).astype(BF16)
            give_back(slot).start()

    def turn(step):
        relay(step - 1)
        ready(step - 1)
        timed("experts", experts, slot_of(step - 1, 0))
        for side in range(2):
            near(slot_of(step - 1, side)).start()

        @pl.when(step + 1 < remote_lines)
        def next_line():
            forward(step + 1)

        send_far(step - 1)

        @pl.when(step >= 2)
        def attend_line():
            attend_step(step - 1)

        kv_step(step)

        @pl.when(step >= 2)
        def answer():
            send_total(step - 2)

    if remote_lines:
        each(1, remote_lines + 1, turn)

    if remote_lines:
        attend_step(remote_lines)
    weights[6].wait()
    rows_out = shard // tp_size
    mixer_term = jnp.dot(
        attended[...].astype(BF16), mixer_w[...], preferred_element_type=F32
    ).astype(BF16)
    for place in range(tp_size):
        high = lax.rem(place // 2 + own_tp // 2, 2)
        low = lax.rem(place + own_tp, 2)
        mix_part[high + 2 * low] = mixer_term[place * rows_out : (place + 1) * rows_out]
    mix_near_copy = send_of(
        mix_part.at[pl.ds(2, 2)], near_mix, small_sems, NEAR_MIX, to_partner
    )
    mix_near_copy.start()

    got("wait_near_shared", shared_near_copy)
    got("wait_pair_back", pair_back)
    far_shared_out[...] = (
        shared_acc[1] + near_shared[1].astype(F32) + mixed(pair_ep, 1, lambda: pair_in[1])
    ).astype(BF16)
    shared_far_copy = send_of(far_shared_out, far_shared, small_sems, FAR_SHARED, to_across)
    shared_far_copy.start()
    got("wait_near_mix", mix_near_copy)
    far_mix_out[...] = (mix_part[1].astype(F32) + near_mix[1].astype(F32)).astype(BF16)
    mix_far_copy = send_of(far_mix_out, far_mix, small_sems, FAR_MIX, to_across)
    mix_far_copy.start()
    if remote_lines:
        send_total(remote_lines - 1)
    result[...] = (
        shared_acc[0] + near_shared[0].astype(F32) + mixed(pair_ep, 0, lambda: pair_in[0])
    )

    def take_back(step):
        for side in range(2):
            slot = slot_to(step, side)
            block = back.at[slot]
            got("wait_back", send_of(block, block, return_sems, slot, here))
            result[...] = result[...] + mixed(to_ep(slot), 0, lambda: back[slot])

    each(0, remote_lines, take_back)
    got("wait_far_shared", shared_far_copy)
    expert_out[...] = result[...] + far_shared[...].astype(F32)
    got("wait_far_mix", mix_far_copy)
    mixer_out[...] = (
        mix_part[0].astype(F32) + near_mix[0].astype(F32) + far_mix[...].astype(F32)
    )

    own_copy(0, 1, 0, to_across).wait_send()
    own_copy(0, 2, 1, to_partner).wait_send()
    own_copy(1, 3, 2, to_partner).wait_send()
    for target, place in ((1, to_across), (2, to_partner), (3, to_diagonal)):
        info_copy(target, target, place).wait_send()
    go(1).wait_send()
    to_side(0, 1, 2, partner_sems, to_partner).wait_send()
    to_side(1, 1, 3, relay_sems, to_partner).wait_send()
    near(1).wait_send()
    for copy in (
        pair_across,
        pair_back,
        shared_near_copy,
        shared_far_copy,
        mix_near_copy,
        mix_far_copy,
    ):
        copy.wait_send()

    def finish(slot):
        go(slot).wait_send()
        to_side(0, slot, 1, across_sems, to_across).wait_send()
        to_side(0, slot, 2, partner_sems, to_partner).wait_send()
        to_side(1, slot, 3, relay_sems, to_partner).wait_send()
        near(slot).wait_send()
        far(slot).wait_send()
        give_back(slot).wait_send()

    each(2, ep_size, finish)

    def finish_kv(step):
        @pl.when((step <= line) & (line + 1 < lines))
        def sent_on():
            kv_line(kv_all.at[2 * step], step + 1).wait_send()

        @pl.when((step <= line) & (step >= 1))
        def sent_over():
            kv_pair(kv_all.at[2 * step], step).wait_send()

    each(0, lines, finish_kv)

    @pl.when(parity == 0)
    def sent_pair():
        kv_pair(kv_ref, 0).wait_send()


def closing_norms(mixer_sum, expert_sum, mixer_gain, exit_gain, mixer_out, expert_out):
    mixer_out[...] = root_norm(mixer_sum[...], mixer_gain[...]).astype(BF16)
    expert_out[...] = root_norm(expert_sum[...], exit_gain[...]).astype(BF16)


def on_device(
    query_rows,
    key_rows,
    value_rows,
    key_bias,
    mixer_weight,
    mixer_gain,
    routed_input,
    entry_gain,
    expert_index,
    route_weights,
    expert_gate,
    expert_up,
    expert_down,
    shared_gate,
    shared_up,
    shared_down,
    exit_gain,
):
    ep_size = lax.axis_size("ep")
    tp_size = lax.axis_size("tp")
    plan = Plan(
        ep_size, tp_size, key_bias.shape[1], query_rows, routed_input, expert_index, expert_gate
    )
    shard, width, model, rows = plan.shard, plan.width, plan.model, plan.rows
    kv_rows = shard + -(-plan.heads // 8) * 8
    small = [
        query_rows,
        key_rows,
        value_rows,
        jnp.transpose(key_bias),
        routed_input,
        entry_gain.reshape(1, model),
        jnp.transpose(expert_index),
        jnp.transpose(route_weights),
    ]
    large = [
        mixer_weight,
        expert_gate,
        expert_up,
        expert_down,
        shared_gate,
        shared_up,
        shared_down,
    ]
    vmem = pl.BlockSpec(memory_space=pltpu.VMEM)
    block = (plan.block, plan.half)
    mix = (shard // tp_size, model)

    def buffer(*shape, kind=BF16):
        return pltpu.VMEM(shape, kind)

    scratch = [pltpu.VMEM(value.shape, value.dtype) for value in large]
    scratch += [
        buffer(tp_size, rows, model),
        buffer(tp_size, 8, plan.padded_rows, kind=F32),
        buffer(tp_size, plan.padded_rows, 128, kind=F32),
        buffer(ep_size, *block),
        buffer(*block),
        buffer(ep_size, tp_size, *block),
        buffer(ep_size, tp_size, *block),
        buffer(ep_size, 2, *block),
        buffer(ep_size, *block),
        buffer(ep_size, *block),
        buffer(ep_size, *block),
        buffer(ep_size, *block),
        buffer(2, *block),
        buffer(2, *block),
        buffer(tp_size, rows, model, kind=F32),
        buffer(2, rows, model),
        buffer(2, rows, model),
        buffer(rows, model),
        buffer(rows, model),
        buffer(rows, model, kind=F32),
        buffer(tp_size, *mix),
        buffer(2, *mix),
        buffer(*mix),
        buffer(*mix),
        buffer(kv_rows, 2 * width),
        buffer(ep_size, kv_rows, 2 * width),
        buffer(plan.heads * shard, width),
        buffer(plan.heads * shard, shard, kind=F32),
        buffer(shard, width, kind=F32),
    ]
    sem = pltpu.SemaphoreType.DMA
    scratch += [sem((len(large),))]
    for count in (4, 4, ep_size, ep_size, ep_size, ep_size, ep_size, ep_size, ep_size, ep_size, ep_size, 6):
        scratch += [sem((count,)), sem((count,))]
    mixer_sum, expert_sum = pl.pallas_call(
        functools.partial(layer_kernel, plan),
        out_shape=(
            jax.ShapeDtypeStruct(mix, F32),
            jax.ShapeDtypeStruct((rows, model), F32),
        ),
        in_specs=[vmem] * len(small) + [pl.BlockSpec(memory_space=pl.ANY)] * len(large),
        out_specs=(vmem, vmem),
        scratch_shapes=scratch,
        compiler_params=pltpu.CompilerParams(
            collective_id=0, has_side_effects=True, vmem_limit_bytes=62 * 1024 * 1024
        ),
        name="whole_layer",
    )(*small, *large)
    return pl.pallas_call(
        closing_norms,
        out_shape=(
            jax.ShapeDtypeStruct(mix, BF16),
            jax.ShapeDtypeStruct((rows, model), BF16),
        ),
        in_specs=[vmem] * 4,
        out_specs=(vmem, vmem),
        name="closing_norms",
    )(mixer_sum, expert_sum, mixer_gain.reshape(1, model), exit_gain.reshape(1, model))


def solution(mesh):
    in_specs = (
        P("ep", "tp"),
        P("ep", "tp"),
        P("ep", "tp"),
        P("ep", "tp"),
        P("tp", None),
        P(),
        P(("ep", "tp"), None),
        P(),
        P(("ep", "tp"), None),
        P(("ep", "tp"), None),
        P("ep", None, "tp"),
        P("ep", None, "tp"),
        P("ep", "tp", None),
        P(None, "tp"),
        P(None, "tp"),
        P("tp", None),
        P(),
    )
    out_specs = (P(("ep", "tp"), None), P(("ep", "tp"), None))
    return jax.shard_map(
        on_device, mesh=mesh, in_specs=in_specs, out_specs=out_specs, check_vma=False
    )
```

```python
import functools

import jax
import jax.numpy as jnp
from jax import lax
from jax.experimental import pallas as pl
from jax.experimental.pallas import tpu as pltpu
from jax.sharding import PartitionSpec as P

MESH = pl.DeviceIdType.MESH
EPS = 1e-06
F32 = jnp.float32
BF16 = jnp.bfloat16
STRAIGHT = (0,)


class Plan:
    def __init__(self, ep_size, tp_size, head_count, query, rows, index, gate):
        self.ep = ep_size
        self.tp = tp_size
        self.lines = ep_size // 2
        self.heads = head_count
        self.shard, self.width = query.shape
        self.head_size = self.width // head_count
        self.rows, self.model = rows.shape
        self.half = self.model // 2
        self.top = index.shape[1]
        self.local = gate.shape[0]
        self.hidden = gate.shape[2]
        self.experts = self.local * ep_size
        self.capacity = 3 * self.rows * self.top // (2 * self.experts)
        self.main = self.capacity // 16 * 16
        self.tail = self.capacity - self.main
        self.block_main = self.local * self.main
        self.block_tail = self.local * self.tail
        self.picked = self.block_main + 2 * self.block_tail
        self.block = 2 * self.block_main + 2 * self.block_tail
        self.named = -(-self.experts // 16) * 16
        self.padded_rows = -(-self.rows // 128) * 128


def send_of(source, target, sems, slot, place):
    return pltpu.make_async_remote_copy(
        src_ref=source,
        dst_ref=target,
        send_sem=sems[0].at[slot],
        recv_sem=sems[1].at[slot],
        device_id=place,
        device_id_type=MESH,
    )


def got(name, copy):
    with jax.named_scope(name):
        copy.wait_recv()


def timed(name, action, *args):
    with jax.named_scope(name):
        return action(*args)


def iota(shape, axis):
    return lax.broadcasted_iota(jnp.int32, shape, axis)


def root_norm(values, gain_row):
    return values * lax.rsqrt(jnp.mean(values * values, axis=-1, keepdims=True) + EPS) * gain_row


def silu(value):
    return value / (1.0 + jnp.exp(-value))


def tail_code(plan, place):
    row = lax.rem(place, plan.block_tail)
    return row // plan.tail * plan.capacity + plan.main + lax.rem(row, plan.tail)


def picked_code(plan, place):
    if plan.main == 0:
        return tail_code(plan, place)
    code = place // plan.main * plan.capacity + lax.rem(place, plan.main)
    if plan.tail == 0:
        return code
    after = jnp.maximum(place - plan.block_main, 0)
    return jnp.where(place < plan.block_main, code, tail_code(plan, after))


def block_code(plan, place):
    bm = plan.block_main
    if bm == 0:
        return tail_code(plan, place), place // plan.block_tail
    row = lax.rem(place, bm)
    code = row // plan.main * plan.capacity + lax.rem(row, plan.main)
    side = place // bm
    if plan.tail == 0:
        return code, side
    after = jnp.maximum(place - 2 * bm, 0)
    is_tail = place >= 2 * bm
    return (
        jnp.where(is_tail, tail_code(plan, after), code),
        jnp.where(is_tail, after // plan.block_tail, side),
    )


def layer_kernel(plan, *refs):
    (
        input_hbm,
        entry_hbm,
        index_hbm,
        route_hbm,
        key_hbm,
        value_hbm,
        bias_hbm,
        query_hbm,
        exit_hbm,
        mixer_gain_hbm,
        mixer_hbm,
        gate_hbm,
        up_hbm,
        down_hbm,
        shared_gate_hbm,
        shared_up_hbm,
        shared_down_hbm,
        mixer_out,
        expert_out,
        input_ref,
        entry_ref,
        index_ref,
        route_ref,
        key_ref,
        value_ref,
        bias_ref,
        query_ref,
        exit_ref,
        mixer_gain_ref,
        mixer_w,
        gate_w,
        up_w,
        down_w,
        shared_gate_w,
        shared_up_w,
        shared_down_w,
        across_rows,
        own_all,
        info,
        info_cols,
        out,
        out_pair,
        arrived,
        part,
        near_in,
        far_out,
        far_in,
        total,
        back,
        pair_out,
        pair_in,
        twin_out,
        twin_in,
        shared_acc,
        shared_near,
        near_shared,
        far_shared_out,
        far_shared,
        result,
        mix_part,
        near_mix,
        far_mix_out,
        far_mix,
        kv_ref,
        kv_all,
        query_heads,
        carried,
        attended,
        input_sem,
        weight_sem,
        own_send,
        own_recv,
        info_send,
        info_recv,
        kv_line_send,
        kv_line_recv,
        kv_pair_send,
        kv_pair_recv,
        go_send,
        go_recv,
        across_send,
        across_recv,
        partner_send,
        partner_recv,
        relay_send,
        relay_recv,
        near_send,
        near_recv,
        far_send,
        far_recv,
        return_send,
        return_recv,
        small_send,
        small_recv,
    ) = refs
    ep_size, tp_size, lines = plan.ep, plan.tp, plan.lines
    rows_n, half = plan.rows, plan.half
    bm = plan.block_main
    own_ep = lax.axis_index("ep")
    own_tp = lax.axis_index("tp")
    partner_tp = own_tp + 1 - 2 * lax.rem(own_tp, 2)
    across_tp = lax.rem(own_tp + tp_size // 2, tp_size)
    diagonal_tp = lax.rem(partner_tp + tp_size // 2, tp_size)
    line = own_ep // 2
    parity = lax.rem(own_ep, 2)
    pair_ep = own_ep + 1 - 2 * parity
    to_across = (own_ep, across_tp)
    to_partner = (own_ep, partner_tp)
    to_diagonal = (own_ep, diagonal_tp)
    to_pair = (pair_ep, own_tp)
    here = (own_ep, own_tp)

    own_sems = (own_send, own_recv)
    info_sems = (info_send, info_recv)
    kv_line_sems = (kv_line_send, kv_line_recv)
    kv_pair_sems = (kv_pair_send, kv_pair_recv)
    go_sems = (go_send, go_recv)
    across_sems = (across_send, across_recv)
    partner_sems = (partner_send, partner_recv)
    relay_sems = (relay_send, relay_recv)
    near_sems = (near_send, near_recv)
    far_sems = (far_send, far_recv)
    return_sems = (return_send, return_recv)
    small_sems = (small_send, small_recv)
    PAIR_ACROSS, PAIR_BACK, NEAR_SHARED, FAR_SHARED, NEAR_MIX, FAR_MIX, TWIN = range(7)

    def to_ep(slot):
        return 2 * lax.rem(line + slot // 2, lines) + lax.rem(parity + slot, 2)

    def from_ep(slot):
        return 2 * lax.rem(line - slot // 2 + lines, lines) + lax.rem(parity + slot, 2)

    def each(first, last, action):
        lax.fori_loop(first, last, lambda step, c: (action(step), c)[1], 0)

    remote_lines = lines - 1

    def other_line(step):
        middle = lines // 2
        inner = jnp.minimum(line, lines - 1 - line)
        index = jnp.where(step <= middle + inner - 1, step - 1, step)
        around = index < 2 * inner
        distance = jnp.where(around, index // 2 + 1, index - inner + 1)
        to_end = jnp.where(around, lax.rem(index, 2), 1)
        upward = (2 * line < lines) == (to_end == 1)
        near_line = jnp.where(upward, line + distance, line - distance)
        return jnp.where(step == 0, lax.rem(line + middle, lines), near_line)

    twin = line + 1 - 2 * lax.rem(line, 2)
    twin_from = 2 * lax.rem(line - twin + lines, lines)
    twin_to = 2 * lax.rem(twin - line + lines, lines)

    def slot_of(step, side):
        return 2 * lax.rem(line - other_line(step) + lines, lines) + side

    def slot_to(step, side):
        return 2 * lax.rem(other_line(step) - line + lines, lines) + side

    barrier = pltpu.get_barrier_semaphore()

    def greet(step):
        place = lax.rem(own_ep + step, ep_size)
        pl.semaphore_signal(barrier, inc=1, device_id=(place, own_tp), device_id_type=MESH)

    each(1, ep_size, greet)
    for place in (partner_tp, across_tp, diagonal_tp):
        pl.semaphore_signal(barrier, inc=1, device_id=(own_ep, place), device_id_type=MESH)

    inputs = [
        pltpu.make_async_copy(source, target, input_sem.at[number])
        for number, (source, target) in enumerate(
            [
                (input_hbm, input_ref),
                (entry_hbm, entry_ref),
                (index_hbm, index_ref),
                (route_hbm, route_ref),
                (key_hbm, key_ref),
                (value_hbm, value_ref),
                (bias_hbm, bias_ref),
                (query_hbm, query_ref),
                (exit_hbm, exit_ref),
                (mixer_gain_hbm, mixer_gain_ref),
            ]
        )
    ]
    for copy in inputs:
        copy.start()

    weights = [
        pltpu.make_async_copy(source, target, weight_sem.at[number])
        for number, (source, target) in enumerate(
            [
                (shared_gate_hbm, shared_gate_w),
                (shared_up_hbm, shared_up_w),
                (shared_down_hbm, shared_down_w),
                (gate_hbm, gate_w),
                (up_hbm, up_w),
                (down_hbm, down_w),
                (mixer_hbm, mixer_w),
            ]
        )
    ]
    for copy in weights:
        copy.start()

    inputs[0].wait()
    with jax.named_scope("wait_barrier"):
        pl.semaphore_wait(barrier, ep_size - 1 + 3)

    def own_copy(source, target, number, place):
        return send_of(own_all.at[source], own_all.at[target], own_sems, number, place)

    rows_over_x = send_of(input_ref, across_rows, own_sems, 0, to_across)
    rows_over_x.start()

    def entry_norm(ref):
        return root_norm(ref[...].astype(F32), entry_ref[...]).astype(BF16)

    for copy in inputs[1:4]:
        copy.wait()
    normed = entry_norm(input_ref)
    own_all[0] = normed
    own_copy(0, 2, 1, to_partner).start()

    expert_at = iota((plan.named, rows_n), 0)
    named = [expert_at == index_ref[k : k + 1] for k in range(plan.top)]
    both = jnp.zeros((plan.named, rows_n), F32)
    for one in named:
        both = both + jnp.where(one, 1.0, 0.0)
    earlier = jnp.where(iota((rows_n, rows_n), 0) < iota((rows_n, rows_n), 1), 1.0, 0.0)
    rank = jnp.dot(both.astype(BF16), earlier.astype(BF16), preferred_element_type=F32)
    rank = rank + expert_at.astype(F32) * plan.capacity
    info[0] = jnp.zeros_like(info[0])
    for k, one in enumerate(named):
        code = jnp.sum(jnp.where(one, rank, 0.0), axis=0, keepdims=True)
        info[0, k : k + 1, 0:rows_n] = code
        info[0, plan.top + k : plan.top + k + 1, 0:rows_n] = route_ref[k : k + 1]

    def turned(value):
        return jnp.transpose(value, (1, 0))

    def picks(codes, rel):
        hit = codes == info[rel, 0:1, 0:rows_n]
        for k in range(1, plan.top):
            hit = hit | (codes == info[rel, k : k + 1, 0:rows_n])
        return jnp.where(hit, 1.0, 0.0).astype(BF16)

    def pack(chosen, put):
        if bm:
            put(0, bm, chosen[0:bm, 0:half])
            put(bm, 2 * bm, chosen[0:bm, half:])
        if plan.block_tail:
            side = iota((2 * plan.block_tail, half), 0) // plan.block_tail
            value = jnp.where(side == 0, chosen[bm:, 0:half], chosen[bm:, half:])
            put(2 * bm, plan.block, value)

    per_block = plan.local * plan.capacity
    picked_rows = iota((ep_size * plan.picked, 1), 0)
    picked_slot = picked_rows // plan.picked
    codes = to_ep(picked_slot) * per_block + picked_code(
        plan, lax.rem(picked_rows, plan.picked)
    )
    chosen = jnp.dot(picks(codes.astype(F32), 0), normed, preferred_element_type=F32)
    for slot in range(ep_size):

        def put_out(first, last, value, slot=slot):
            out[slot, first:last] = value.astype(BF16)

        pack(chosen[slot * plan.picked : (slot + 1) * plan.picked], put_out)

    for copy in inputs[4:]:
        copy.wait()
    shard, width, heads = plan.shard, plan.width, plan.heads
    kv_ref[0:shard, 0:width] = key_ref[...]
    kv_ref[0:shard, width:] = value_ref[...]
    kv_ref[shard:] = jnp.zeros((kv_ref.shape[0] - shard, 2 * width), BF16)
    kv_ref[shard : shard + heads, 0:shard] = bias_ref[...]

    def info_copy(target, number, place):
        return send_of(info.at[0], info.at[target], info_sems, number, place)

    def go(slot):
        return send_of(
            out.at[slot], arrived.at[slot, 0], go_sems, slot, (to_ep(slot), own_tp)
        )

    def kv_line(source, step):
        return send_of(
            source, kv_all.at[2 * step], kv_line_sems, step, (own_ep + 2, own_tp)
        )

    def kv_pair(source, step):
        return send_of(source, kv_all.at[2 * step + 1], kv_pair_sems, step, to_pair)

    for target, place in ((1, to_across), (2, to_partner), (3, to_diagonal)):
        info_copy(target, target, place).start()
    go(1).start()

    def go_line(step):
        go(slot_to(step, 0)).start()
        go(slot_to(step, 1)).start()

    early = max(remote_lines - 1, 0)
    each(0, early, go_line)

    @pl.when(line + 1 < lines)
    def kv_first():
        kv_line(kv_ref, 1).start()

    each(early, remote_lines, go_line)

    @pl.when(parity == 0)
    def kv_to_pair():
        kv_pair(kv_ref, 0).start()

    head_of = iota((shard, width), 1) // plan.head_size
    queries = query_ref[...].astype(F32) * plan.head_size ** (-0.5)
    for head in range(heads):
        query_heads[head * shard : (head + 1) * shard] = jnp.where(
            head_of == head, queries, 0.0
        ).astype(BF16)
    attended[...] = jnp.zeros_like(attended)
    carried[...] = jnp.zeros_like(carried)

    def attend_block(load, own):
        keys = load(slice(0, shard), slice(0, width))
        values = load(slice(0, shard), slice(width, 2 * width))
        bias = load(slice(shard, shard + heads), slice(0, shard)).astype(F32)
        deep = (2 * shard, 2 * shard)
        row_key, column_key = lax.rem(iota(deep, 0), shard), iota(deep, 1)
        later_of = jnp.where((row_key > column_key) | (column_key >= shard), 1.0, 0.0)
        later_of = later_of.astype(BF16)
        before = iota((shard, shard), 1) < iota((shard, shard), 0)
        scores = lax.dot_general(
            query_heads[...], keys, (((1,), (1,)), ((), ())), preferred_element_type=F32
        )
        gained = attended[...]
        for head in range(heads):
            rows = slice(head * shard, (head + 1) * shard)
            score = scores[rows] + bias[head : head + 1]
            fails = -(jnp.maximum(score, 0.0) + jnp.log(1.0 + jnp.exp(-jnp.abs(score))))
            if own:
                hits = score + fails
                fails = jnp.where(before, fails, 0.0)
            else:
                hits = score + fails
            high = fails.astype(BF16)
            low = (fails - high.astype(F32)).astype(BF16)
            sums = jnp.dot(
                jnp.concatenate([high, low], axis=1), later_of, preferred_element_type=F32
            )
            taken = carried[rows]
            weights = jnp.exp(hits + sums[:, 0:shard] + taken)
            if own:
                weights = jnp.where(before, weights, 0.0)
            product = jnp.dot(weights.astype(BF16), values, preferred_element_type=F32)
            gained = gained + jnp.where(head_of == head, product, 0.0)
            carried[rows] = taken + sums[:, shard : 2 * shard]
        attended[...] = gained

    timed("attend_own", attend_block, lambda rows, cols: kv_ref[rows, cols], True)

    def attend_slot(slot):
        attend_block(lambda rows, cols: kv_all[slot, rows, cols], False)

    def kv_step(step):
        @pl.when(step <= line)
        def one():
            block = kv_all.at[2 * step]
            got("wait_kv_line", send_of(block, block, kv_line_sems, step, here))

            @pl.when(line + 1 < lines)
            def further():
                kv_line(block, step + 1).start()

            kv_pair(block, step).start()

    def attend_step(step):
        @pl.when(step <= line)
        def one():
            other = kv_all.at[2 * step + 1]
            got("wait_kv_pair", send_of(other, other, kv_pair_sems, step, here))

            def turn(side, c):
                timed("attend", attend_slot, 2 * step + lax.rem(side + 1 - parity, 2))
                return c

            lax.fori_loop(0, 2, turn, 0)

    def landed(slot):
        block = arrived.at[slot, 0]
        return send_of(block, block, go_sems, slot, here)

    def to_side(rel, slot, target, sems, place):
        return send_of(arrived.at[slot, rel], arrived.at[slot, target], sems, slot, place)

    got("wait_pair", landed(1))
    to_side(0, 1, 2, partner_sems, to_partner).start()

    got("wait_own_across", rows_over_x)
    own_all[1] = entry_norm(across_rows)
    own_copy(1, 3, 2, to_partner).start()
    info_copy(1, 1, here).wait_recv()

    def choose(target_ep, rel, put):
        place = iota((plan.picked, 1), 0)
        codes = target_ep * per_block + picked_code(plan, place)
        pack(
            jnp.dot(picks(codes.astype(F32), rel), own_all[rel], preferred_element_type=F32), put
        )

    def put_pair(first, last, value):
        out_pair[first:last] = value.astype(BF16)

    choose(pair_ep, 1, put_pair)
    pair_across = send_of(out_pair, arrived.at[1, 1], small_sems, PAIR_ACROSS, to_pair)
    pair_across.start()

    def forward_side(step, side):
        slot = slot_of(step, side)
        got("wait_landed", landed(slot))
        to_side(0, slot, 1, across_sems, to_across).start()
        to_side(0, slot, 2, partner_sems, to_partner).start()

    def forward(step):
        for side in range(2):
            forward_side(step, side)

    if remote_lines:
        forward_side(0, 0)

    def relay(step, side):
        slot = slot_of(step, side)
        got("wait_across", to_side(1, slot, 1, across_sems, here))
        to_side(1, slot, 3, relay_sems, to_partner).start()

    got("wait_own_partner", own_copy(2, 2, 1, here))
    got("wait_own_diag", own_copy(3, 3, 2, here))
    for rel in (2, 3):
        info_copy(rel, rel, here).wait_recv()
    for rel in range(tp_size):
        info_cols[rel, :, 0:8] = turned(info[rel])
    for copy in weights[0:3]:
        copy.wait()

    def shared_expert():
        shared_rows = own_all[...].reshape(tp_size * rows_n, plan.model)
        hidden = silu(jnp.dot(shared_rows, shared_gate_w[...], preferred_element_type=F32))
        hidden = hidden * jnp.dot(shared_rows, shared_up_w[...], preferred_element_type=F32)
        shared_acc[...] = jnp.dot(
            hidden.astype(BF16), shared_down_w[...], preferred_element_type=F32
        ).reshape(shared_acc.shape)

    timed("shared", shared_expert)
    if remote_lines:
        forward_side(0, 1)

    def put_own(first, last, value, rel):
        arrived[0, rel, first:last] = value.astype(BF16)

    def choose_own():
        arrived[0, 0] = out[0]
        for rel in (1, 2, 3):
            choose(own_ep, rel, functools.partial(put_own, rel=rel))

    timed("choose_own", choose_own)

    blocks = 2 * tp_size
    tails = blocks * plan.tail
    folded = blocks * 2 * plan.block_tail

    def tail_move(side, by_column):
        shape = (folded, plan.local * tails) if by_column else (plan.local * tails, folded)
        sorted_at = iota(shape, 1 if by_column else 0)
        folded_at = iota(shape, 0 if by_column else 1)
        expert = sorted_at // tails
        block = lax.rem(sorted_at, tails) // plan.tail
        spot = lax.rem(sorted_at, plan.tail)
        target = (
            block * 2 * plan.block_tail + side * plan.block_tail + expert * plan.tail + spot
        )
        return jnp.where(folded_at == target, 1.0, 0.0).astype(BF16)

    def experts(first):
        pair = arrived.at[pl.ds(first, 2)]
        tail_rows = None
        if plan.tail:
            folded_rows = pair[:, :, 2 * bm : plan.block].reshape(folded, half)
            tail_rows = jnp.concatenate(
                [
                    jnp.dot(tail_move(side, False), folded_rows, preferred_element_type=F32)
                    for side in range(2)
                ],
                axis=1,
            ).astype(BF16)
        tail_results = []
        for expert in range(plan.local):
            pieces = []
            if plan.main:
                at = expert * plan.main
                left = pair[:, :, at : at + plan.main]
                right = pair[:, :, bm + at : bm + at + plan.main]
                pieces.append(
                    jnp.concatenate([left, right], axis=3).reshape(
                        blocks * plan.main, plan.model
                    )
                )
            if plan.tail:
                pieces.append(tail_rows[expert * tails : (expert + 1) * tails])
            x = pieces[0] if len(pieces) == 1 else jnp.concatenate(pieces, axis=0)
            hidden = silu(jnp.dot(x, gate_w[expert], preferred_element_type=F32))
            hidden = hidden * jnp.dot(x, up_w[expert], preferred_element_type=F32)
            result_rows = jnp.dot(
                hidden.astype(BF16), down_w[expert], preferred_element_type=F32
            ).astype(BF16)
            if plan.main:
                at = expert * plan.main
                shape = (2, tp_size, plan.main, half)
                count = blocks * plan.main
                part[pl.ds(first, 2), :, at : at + plan.main] = result_rows[
                    0:count, 0:half
                ].reshape(shape)
                part[pl.ds(first, 2), :, bm + at : bm + at + plan.main] = result_rows[
                    0:count, half:
                ].reshape(shape)
            if plan.tail:
                tail_results.append(result_rows[blocks * plan.main :])
        if plan.tail:
            ends = jnp.concatenate(tail_results, axis=0)
            value = jnp.dot(
                tail_move(0, True), ends[:, 0:half], preferred_element_type=F32
            ) + jnp.dot(tail_move(1, True), ends[:, half:], preferred_element_type=F32)
            part[pl.ds(first, 2), :, 2 * bm : plan.block] = value.astype(BF16).reshape(
                2, tp_size, 2 * plan.block_tail, half
            )

    def mixed(target_ep, rel, load):
        place = iota((1, plan.block), 1)
        code, side = block_code(plan, place)
        code = (code + target_ep * per_block).astype(F32)
        weight = jnp.zeros((rows_n, plan.block), F32)
        for k in range(plan.top):
            hit = code == info_cols[rel, 0:rows_n, k : k + 1]
            at = plan.top + k
            weight = weight + jnp.where(hit, info_cols[rel, 0:rows_n, at : at + 1], 0.0)
        sums = []
        for which in range(2):
            kept = jnp.where(side == which, weight, 0.0)
            high = kept.astype(BF16)
            low = (kept - high.astype(F32)).astype(BF16)
            value = jnp.dot(
                jnp.concatenate([high, low], axis=0), load(), preferred_element_type=F32
            )
            sums.append(value[0:rows_n] + value[rows_n:])
        return jnp.concatenate(sums, axis=1)

    def near(slot):
        return send_of(
            part.at[slot, pl.ds(2, 2)], near_in.at[slot], near_sems, slot, to_partner
        )

    block = arrived.at[1, 1]
    got("wait_pair_across", send_of(block, block, small_sems, PAIR_ACROSS, here))
    to_side(1, 1, 3, relay_sems, to_partner).start()
    got("wait_pair_p", to_side(2, 1, 2, partner_sems, here))
    got("wait_pair_r", to_side(3, 1, 3, relay_sems, here))
    for copy in weights[3:6]:
        copy.wait()
    timed("experts_own", experts, 0)
    near(1).start()
    if remote_lines > 1:
        forward(1)

    def fold_own():
        for rel in range(tp_size):
            shared_acc[rel] = shared_acc[rel] + mixed(own_ep, rel, lambda rel=rel: part[0, rel])

    timed("fold_own", fold_own)
    if remote_lines:
        relay(0, 0)
    shared_near[...] = shared_acc[2:4].astype(BF16)
    shared_near_copy = send_of(shared_near, near_shared, small_sems, NEAR_SHARED, to_partner)
    shared_near_copy.start()
    got("wait_near1", near(1))
    pair_out[...] = (part[1, 0:2].astype(F32) + near_in[1].astype(F32)).astype(BF16)
    pair_back = send_of(pair_out, pair_in, small_sems, PAIR_BACK, to_pair)
    pair_back.start()

    @pl.when(parity == 1)
    def attend_pair():
        block = kv_all.at[1]
        got("wait_kv_pair", send_of(block, block, kv_pair_sems, 0, here))
        timed("attend", attend_slot, 1)

    if remote_lines:
        kv_step(1)


    def ready(step):
        for side in range(2):
            slot = slot_of(step, side)
            got("wait_partner", to_side(2, slot, 2, partner_sems, here))
            got("wait_relay", to_side(3, slot, 3, relay_sems, here))

    def far(slot):
        return send_of(far_out.at[slot], far_in.at[slot], far_sems, slot, to_across)

    def twin_copy(side):
        return send_of(
            twin_out.at[side],
            twin_in.at[side],
            small_sems,
            TWIN + side,
            (from_ep(twin_from + side), own_tp),
        )

    def send_far(step):
        is_twin = other_line(step) == twin
        for side in range(2):
            slot = slot_of(step, side)
            got("wait_near", near(slot))

            def over_x(slot=slot):
                value = part[slot, 1].astype(F32) + near_in[slot, 1].astype(F32)
                far_out[slot] = value.astype(BF16)
                far(slot).start()

            def straight(slot=slot, side=side):
                value = part[slot, 0:2].astype(F32) + near_in[slot].astype(F32)
                twin_out[side] = value.astype(BF16)
                twin_copy(side).start()

            if side in STRAIGHT:
                pl.when(is_twin)(straight)
                pl.when(jnp.logical_not(is_twin))(over_x)
            else:
                over_x()

    def give_back(slot):
        return send_of(
            total.at[slot], back.at[slot], return_sems, slot, (from_ep(slot), own_tp)
        )

    def send_total(step):
        def reduced(slot):
            got("wait_far", far(slot))
            total[slot] = (
                part[slot, 0].astype(F32)
                + near_in[slot, 0].astype(F32)
                + far_in[slot].astype(F32)
            ).astype(BF16)
            give_back(slot).start()

        for side in range(2):
            if side in STRAIGHT:
                pl.when(other_line(step) != twin)(
                    functools.partial(reduced, slot_of(step, side))
                )
            else:
                reduced(slot_of(step, side))

    def turn(step):
        @pl.when(step >= 2)
        def relay_first():
            relay(step - 1, 0)

        relay(step - 1, 1)

        @pl.when(step >= 3)
        def attend_line():
            attend_step(step - 2)

        ready(step - 1)
        timed("experts", experts, slot_of(step - 1, 0))
        for side in range(2):
            near(slot_of(step - 1, side)).start()

        send_far(step - 1)

        @pl.when(step + 1 < remote_lines)
        def next_line():
            forward(step + 1)

        kv_step(step + 1)

        @pl.when(step >= 2)
        def answer():
            send_total(step - 2)

    if remote_lines:
        each(1, remote_lines + 1, turn)

    def folded_rows(rel):
        value = shared_acc[rel] + near_shared[rel].astype(F32)
        value = value + mixed(pair_ep, rel, lambda: pair_in[rel])
        if remote_lines:
            for side in STRAIGHT:
                value = value + mixed(
                    to_ep(twin_to + side), rel, lambda side=side: twin_in[side, rel]
                )
        return value

    got("wait_near_shared", shared_near_copy)
    got("wait_pair_back", pair_back)
    if remote_lines:
        for side in STRAIGHT:
            got("wait_twin", twin_copy(side))
    far_shared_out[...] = folded_rows(1).astype(BF16)
    shared_far_copy = send_of(far_shared_out, far_shared, small_sems, FAR_SHARED, to_across)
    shared_far_copy.start()
    each(max(remote_lines - 1, 1), remote_lines + 1, attend_step)
    weights[6].wait()
    rows_out = shard // tp_size
    mixer_term = jnp.dot(
        attended[...].astype(BF16), mixer_w[...], preferred_element_type=F32
    ).astype(BF16)
    for place in range(tp_size):
        high = lax.rem(place // 2 + own_tp // 2, 2)
        low = lax.rem(place + own_tp, 2)
        mix_part[high + 2 * low] = mixer_term[place * rows_out : (place + 1) * rows_out]
    mix_near_copy = send_of(
        mix_part.at[pl.ds(2, 2)], near_mix, small_sems, NEAR_MIX, to_partner
    )
    mix_near_copy.start()
    if remote_lines:
        send_total(remote_lines - 1)
    got("wait_near_mix", mix_near_copy)
    far_mix_out[...] = (mix_part[1].astype(F32) + near_mix[1].astype(F32)).astype(BF16)
    mix_far_copy = send_of(far_mix_out, far_mix, small_sems, FAR_MIX, to_across)
    mix_far_copy.start()
    result[...] = folded_rows(0)

    rows_over_x.wait_send()
    own_copy(0, 2, 1, to_partner).wait_send()
    own_copy(1, 3, 2, to_partner).wait_send()
    for target, place in ((1, to_across), (2, to_partner), (3, to_diagonal)):
        info_copy(target, target, place).wait_send()
    go(1).wait_send()
    to_side(0, 1, 2, partner_sems, to_partner).wait_send()
    to_side(1, 1, 3, relay_sems, to_partner).wait_send()
    near(1).wait_send()
    for copy in (pair_across, pair_back, shared_near_copy, mix_near_copy):
        copy.wait_send()

    def is_straight(slot):
        found = slot < 0
        for side in STRAIGHT:
            found = found | (slot == twin_from + side)
        return found

    def finish(slot):
        go(slot).wait_send()
        to_side(0, slot, 1, across_sems, to_across).wait_send()
        to_side(0, slot, 2, partner_sems, to_partner).wait_send()
        to_side(1, slot, 3, relay_sems, to_partner).wait_send()
        near(slot).wait_send()

        @pl.when(jnp.logical_not(is_straight(slot)))
        def reduced():
            far(slot).wait_send()

    each(2, ep_size, finish)

    if remote_lines:
        for side in STRAIGHT:
            twin_copy(side).wait_send()

    def finish_kv(step):
        @pl.when((step <= line) & (line + 1 < lines))
        def sent_on():
            kv_line(kv_all.at[2 * step], step + 1).wait_send()

        @pl.when((step <= line) & (step >= 1))
        def sent_over():
            kv_pair(kv_all.at[2 * step], step).wait_send()

    each(0, lines, finish_kv)

    @pl.when(parity == 0)
    def sent_pair():
        kv_pair(kv_ref, 0).wait_send()

    def take_back(step):
        def one(slot):
            block = back.at[slot]
            got("wait_back", send_of(block, block, return_sems, slot, here))
            result[...] = result[...] + mixed(to_ep(slot), 0, lambda: back[slot])

        for side in range(2):
            if side in STRAIGHT:
                pl.when(other_line(step) != twin)(functools.partial(one, slot_to(step, side)))
            else:
                one(slot_to(step, side))

    each(0, remote_lines, take_back)

    def returned(slot):
        @pl.when(jnp.logical_not(is_straight(slot)))
        def one():
            give_back(slot).wait_send()

    each(2, ep_size, returned)
    got("wait_far_shared", shared_far_copy)
    combined = result[...] + far_shared[...].astype(F32)
    expert_out[...] = root_norm(combined, exit_ref[...]).astype(BF16)
    got("wait_far_mix", mix_far_copy)
    mixer_sum = mix_part[0].astype(F32) + near_mix[0].astype(F32) + far_mix[...].astype(F32)
    mixer_out[...] = root_norm(mixer_sum, mixer_gain_ref[...]).astype(BF16)
    shared_far_copy.wait_send()
    mix_far_copy.wait_send()


def hand_on(mixer_in, expert_in, mixer_out, expert_out):
    mixer_out[...] = mixer_in[...]
    expert_out[...] = expert_in[...]


def on_device(
    query_rows,
    key_rows,
    value_rows,
    key_bias,
    mixer_weight,
    mixer_gain,
    routed_input,
    entry_gain,
    expert_index,
    route_weights,
    expert_gate,
    expert_up,
    expert_down,
    shared_gate,
    shared_up,
    shared_down,
    exit_gain,
):
    ep_size = lax.axis_size("ep")
    tp_size = lax.axis_size("tp")
    plan = Plan(
        ep_size, tp_size, key_bias.shape[1], query_rows, routed_input, expert_index, expert_gate
    )
    shard, width, model, rows = plan.shard, plan.width, plan.model, plan.rows
    kv_rows = shard + -(-plan.heads // 8) * 8
    small = [
        routed_input,
        entry_gain.reshape(1, model),
        jnp.transpose(expert_index),
        jnp.transpose(route_weights),
        key_rows,
        value_rows,
        jnp.transpose(key_bias),
        query_rows,
        exit_gain.reshape(1, model),
        mixer_gain.reshape(1, model),
    ]
    large = [
        mixer_weight,
        expert_gate,
        expert_up,
        expert_down,
        shared_gate,
        shared_up,
        shared_down,
    ]
    vmem = pl.BlockSpec(memory_space=pltpu.VMEM)
    block = (plan.block, plan.half)
    mix = (shard // tp_size, model)

    def buffer(*shape, kind=BF16):
        return pltpu.VMEM(shape, kind)

    scratch = [pltpu.VMEM(value.shape, value.dtype) for value in small + large]
    scratch += [
        buffer(rows, model),
        buffer(tp_size, rows, model),
        buffer(tp_size, 8, plan.padded_rows, kind=F32),
        buffer(tp_size, plan.padded_rows, 128, kind=F32),
        buffer(ep_size, *block),
        buffer(*block),
        buffer(ep_size, tp_size, *block),
        buffer(ep_size, tp_size, *block),
        buffer(ep_size, 2, *block),
        buffer(ep_size, *block),
        buffer(ep_size, *block),
        buffer(ep_size, *block),
        buffer(ep_size, *block),
        buffer(2, *block),
        buffer(2, *block),
        buffer(2, 2, *block),
        buffer(2, 2, *block),
        buffer(tp_size, rows, model, kind=F32),
        buffer(2, rows, model),
        buffer(2, rows, model),
        buffer(rows, model),
        buffer(rows, model),
        buffer(rows, model, kind=F32),
        buffer(tp_size, *mix),
        buffer(2, *mix),
        buffer(*mix),
        buffer(*mix),
        buffer(kv_rows, 2 * width),
        buffer(ep_size, kv_rows, 2 * width),
        buffer(plan.heads * shard, width),
        buffer(plan.heads * shard, shard, kind=F32),
        buffer(shard, width, kind=F32),
    ]
    sem = pltpu.SemaphoreType.DMA
    scratch += [sem((len(small),)), sem((len(large),))]
    for count in (4, 4, ep_size, ep_size, ep_size, ep_size, ep_size, ep_size, ep_size, ep_size, ep_size, 8):
        scratch += [sem((count,)), sem((count,))]
    results = pl.pallas_call(
        functools.partial(layer_kernel, plan),
        out_shape=(
            jax.ShapeDtypeStruct(mix, BF16),
            jax.ShapeDtypeStruct((rows, model), BF16),
        ),
        in_specs=[pl.BlockSpec(memory_space=pltpu.HBM)] * len(small + large),
        out_specs=(vmem, vmem),
        scratch_shapes=scratch,
        compiler_params=pltpu.CompilerParams(
            collective_id=0, has_side_effects=True, vmem_limit_bytes=62 * 1024 * 1024
        ),
        name="whole_layer",
    )(*small, *large)
    return pl.pallas_call(
        hand_on,
        out_shape=(
            jax.ShapeDtypeStruct(mix, BF16),
            jax.ShapeDtypeStruct((rows, model), BF16),
        ),
        in_specs=[vmem] * 2,
        out_specs=(vmem, vmem),
        name="hand_on",
    )(*results)


def solution(mesh):
    in_specs = (
        P("ep", "tp"),
        P("ep", "tp"),
        P("ep", "tp"),
        P("ep", "tp"),
        P("tp", None),
        P(),
        P(("ep", "tp"), None),
        P(),
        P(("ep", "tp"), None),
        P(("ep", "tp"), None),
        P("ep", None, "tp"),
        P("ep", None, "tp"),
        P("ep", "tp", None),
        P(None, "tp"),
        P(None, "tp"),
        P("tp", None),
        P(),
    )
    out_specs = (P(("ep", "tp"), None), P(("ep", "tp"), None))
    return jax.shard_map(
        on_device, mesh=mesh, in_specs=in_specs, out_specs=out_specs, check_vma=False
    )
```

```python
import functools

import jax
import jax.numpy as jnp
from jax import lax
from jax.experimental import pallas as pl
from jax.experimental.pallas import tpu as pltpu
from jax.sharding import PartitionSpec as P

MESH = pl.DeviceIdType.MESH
EPS = 1e-06
F32 = jnp.float32
BF16 = jnp.bfloat16
STRAIGHT = (0,)


class Plan:
    def __init__(self, ep_size, tp_size, head_count, query, rows, index, gate):
        self.ep = ep_size
        self.tp = tp_size
        self.lines = ep_size // 2
        self.heads = head_count
        self.shard, self.width = query.shape
        self.head_size = self.width // head_count
        self.rows, self.model = rows.shape
        self.half = self.model // 2
        self.top = index.shape[1]
        self.local = gate.shape[0]
        self.hidden = gate.shape[2]
        self.experts = self.local * ep_size
        self.capacity = 3 * self.rows * self.top // (2 * self.experts)
        self.main = self.capacity // 16 * 16
        self.tail = self.capacity - self.main
        self.block_main = self.local * self.main
        self.block_tail = self.local * self.tail
        self.picked = self.block_main + 2 * self.block_tail
        self.block = 2 * self.block_main + 2 * self.block_tail
        self.named = -(-self.experts // 16) * 16
        self.padded_rows = -(-self.rows // 128) * 128


def send_of(source, target, sems, slot, place):
    return pltpu.make_async_remote_copy(
        src_ref=source,
        dst_ref=target,
        send_sem=sems[0].at[slot],
        recv_sem=sems[1].at[slot],
        device_id=place,
        device_id_type=MESH,
    )


def got(name, copy):
    with jax.named_scope(name):
        copy.wait_recv()


def timed(name, action, *args):
    with jax.named_scope(name):
        return action(*args)


def iota(shape, axis):
    return lax.broadcasted_iota(jnp.int32, shape, axis)


def root_norm(values, gain_row):
    return values * lax.rsqrt(jnp.mean(values * values, axis=-1, keepdims=True) + EPS) * gain_row


def silu(value):
    return value / (1.0 + jnp.exp(-value))


def tail_code(plan, place):
    row = lax.rem(place, plan.block_tail)
    return row // plan.tail * plan.capacity + plan.main + lax.rem(row, plan.tail)


def picked_code(plan, place):
    if plan.main == 0:
        return tail_code(plan, place)
    code = place // plan.main * plan.capacity + lax.rem(place, plan.main)
    if plan.tail == 0:
        return code
    after = jnp.maximum(place - plan.block_main, 0)
    return jnp.where(place < plan.block_main, code, tail_code(plan, after))


def block_code(plan, place):
    bm = plan.block_main
    if bm == 0:
        return tail_code(plan, place), place // plan.block_tail
    row = lax.rem(place, bm)
    code = row // plan.main * plan.capacity + lax.rem(row, plan.main)
    side = place // bm
    if plan.tail == 0:
        return code, side
    after = jnp.maximum(place - 2 * bm, 0)
    is_tail = place >= 2 * bm
    return (
        jnp.where(is_tail, tail_code(plan, after), code),
        jnp.where(is_tail, after // plan.block_tail, side),
    )


def layer_kernel(plan, *refs):
    (
        input_hbm,
        entry_hbm,
        index_hbm,
        route_hbm,
        key_hbm,
        value_hbm,
        bias_hbm,
        query_hbm,
        exit_hbm,
        mixer_gain_hbm,
        mixer_hbm,
        gate_hbm,
        up_hbm,
        down_hbm,
        shared_gate_hbm,
        shared_up_hbm,
        shared_down_hbm,
        mixer_hbm_out,
        expert_hbm_out,
        mixer_out,
        expert_out,
        output_sem,
        input_ref,
        entry_ref,
        index_ref,
        route_ref,
        key_ref,
        value_ref,
        bias_ref,
        query_ref,
        exit_ref,
        mixer_gain_ref,
        mixer_w,
        gate_w,
        up_w,
        down_w,
        shared_gate_w,
        shared_up_w,
        shared_down_w,
        across_rows,
        own_all,
        info,
        info_cols,
        out,
        out_pair,
        arrived,
        part,
        near_in,
        far_out,
        far_in,
        total,
        back,
        pair_out,
        pair_in,
        twin_out,
        twin_in,
        shared_acc,
        shared_near,
        near_shared,
        far_shared_out,
        far_shared,
        result,
        mix_part,
        near_mix,
        far_mix_out,
        far_mix,
        kv_ref,
        kv_all,
        query_heads,
        carried,
        attended,
        input_sem,
        weight_sem,
        own_send,
        own_recv,
        info_send,
        info_recv,
        kv_line_send,
        kv_line_recv,
        kv_pair_send,
        kv_pair_recv,
        go_send,
        go_recv,
        across_send,
        across_recv,
        partner_send,
        partner_recv,
        relay_send,
        relay_recv,
        near_send,
        near_recv,
        far_send,
        far_recv,
        return_send,
        return_recv,
        small_send,
        small_recv,
    ) = refs
    ep_size, tp_size, lines = plan.ep, plan.tp, plan.lines
    rows_n, half = plan.rows, plan.half
    bm = plan.block_main
    own_ep = lax.axis_index("ep")
    own_tp = lax.axis_index("tp")
    partner_tp = own_tp + 1 - 2 * lax.rem(own_tp, 2)
    across_tp = lax.rem(own_tp + tp_size // 2, tp_size)
    diagonal_tp = lax.rem(partner_tp + tp_size // 2, tp_size)
    line = own_ep // 2
    parity = lax.rem(own_ep, 2)
    pair_ep = own_ep + 1 - 2 * parity
    to_across = (own_ep, across_tp)
    to_partner = (own_ep, partner_tp)
    to_diagonal = (own_ep, diagonal_tp)
    to_pair = (pair_ep, own_tp)
    here = (own_ep, own_tp)

    own_sems = (own_send, own_recv)
    info_sems = (info_send, info_recv)
    kv_line_sems = (kv_line_send, kv_line_recv)
    kv_pair_sems = (kv_pair_send, kv_pair_recv)
    go_sems = (go_send, go_recv)
    across_sems = (across_send, across_recv)
    partner_sems = (partner_send, partner_recv)
    relay_sems = (relay_send, relay_recv)
    near_sems = (near_send, near_recv)
    far_sems = (far_send, far_recv)
    return_sems = (return_send, return_recv)
    small_sems = (small_send, small_recv)
    PAIR_ACROSS, PAIR_BACK, NEAR_SHARED, FAR_SHARED, NEAR_MIX, FAR_MIX, TWIN = range(7)

    def to_ep(slot):
        return 2 * lax.rem(line + slot // 2, lines) + lax.rem(parity + slot, 2)

    def from_ep(slot):
        return 2 * lax.rem(line - slot // 2 + lines, lines) + lax.rem(parity + slot, 2)

    def each(first, last, action):
        lax.fori_loop(first, last, lambda step, c: (action(step), c)[1], 0)

    remote_lines = lines - 1

    def other_line(step):
        middle = lines // 2
        margin = jnp.minimum(line, lines - 1 - line)
        index = jnp.where(step <= middle + margin - 1, step - 1, step)
        around = index < 2 * margin
        distance = jnp.where(around, index // 2 + 1, index - margin + 1)
        to_end = jnp.where(around, lax.rem(index, 2), 1)
        upward = (2 * line < lines) == (to_end == 1)
        near_line = jnp.where(upward, line + distance, line - distance)
        return jnp.where(step == 0, lax.rem(line + middle, lines), near_line)

    twin = line + 1 - 2 * lax.rem(line, 2)
    twin_from = 2 * lax.rem(line - twin + lines, lines)
    twin_to = 2 * lax.rem(twin - line + lines, lines)
    outer = (lax.rem(line, 2) == 0) == (2 * line < lines)
    inner = jnp.logical_not(outer)

    def slot_of(step, side):
        return 2 * lax.rem(line - other_line(step) + lines, lines) + side

    def slot_to(step, side):
        return 2 * lax.rem(other_line(step) - line + lines, lines) + side

    barrier = pltpu.get_barrier_semaphore()

    def greet(step):
        place = lax.rem(own_ep + step, ep_size)
        pl.semaphore_signal(barrier, inc=1, device_id=(place, own_tp), device_id_type=MESH)

    each(1, ep_size, greet)
    for place in (partner_tp, across_tp, diagonal_tp):
        pl.semaphore_signal(barrier, inc=1, device_id=(own_ep, place), device_id_type=MESH)

    inputs = [
        pltpu.make_async_copy(source, target, input_sem.at[number])
        for number, (source, target) in enumerate(
            [
                (input_hbm, input_ref),
                (entry_hbm, entry_ref),
                (index_hbm, index_ref),
                (route_hbm, route_ref),
                (key_hbm, key_ref),
                (value_hbm, value_ref),
                (bias_hbm, bias_ref),
                (query_hbm, query_ref),
                (exit_hbm, exit_ref),
                (mixer_gain_hbm, mixer_gain_ref),
            ]
        )
    ]
    for copy in inputs:
        copy.start()

    weights = [
        pltpu.make_async_copy(source, target, weight_sem.at[number])
        for number, (source, target) in enumerate(
            [
                (shared_gate_hbm, shared_gate_w),
                (shared_up_hbm, shared_up_w),
                (shared_down_hbm, shared_down_w),
                (gate_hbm, gate_w),
                (up_hbm, up_w),
                (down_hbm, down_w),
                (mixer_hbm, mixer_w),
            ]
        )
    ]
    for copy in weights:
        copy.start()

    inputs[0].wait()
    with jax.named_scope("wait_barrier"):
        pl.semaphore_wait(barrier, ep_size - 1 + 3)

    def own_copy(source, target, number, place):
        return send_of(own_all.at[source], own_all.at[target], own_sems, number, place)

    rows_over_x = send_of(input_ref, across_rows, own_sems, 0, to_across)
    rows_over_x.start()

    def entry_norm(ref):
        return root_norm(ref[...].astype(F32), entry_ref[...]).astype(BF16)

    for copy in inputs[1:4]:
        copy.wait()
    normed = entry_norm(input_ref)
    own_all[0] = normed
    own_copy(0, 2, 1, to_partner).start()

    expert_at = iota((plan.named, rows_n), 0)
    named = [expert_at == index_ref[k : k + 1] for k in range(plan.top)]
    both = jnp.zeros((plan.named, rows_n), F32)
    for one in named:
        both = both + jnp.where(one, 1.0, 0.0)
    earlier = jnp.where(iota((rows_n, rows_n), 0) < iota((rows_n, rows_n), 1), 1.0, 0.0)
    rank = jnp.dot(both.astype(BF16), earlier.astype(BF16), preferred_element_type=F32)
    rank = rank + expert_at.astype(F32) * plan.capacity
    info[0] = jnp.zeros_like(info[0])
    for k, one in enumerate(named):
        code = jnp.sum(jnp.where(one, rank, 0.0), axis=0, keepdims=True)
        info[0, k : k + 1, 0:rows_n] = code
        info[0, plan.top + k : plan.top + k + 1, 0:rows_n] = route_ref[k : k + 1]

    def turned(value):
        return jnp.transpose(value, (1, 0))

    def picks(codes, rel):
        hit = codes == info[rel, 0:1, 0:rows_n]
        for k in range(1, plan.top):
            hit = hit | (codes == info[rel, k : k + 1, 0:rows_n])
        return jnp.where(hit, 1.0, 0.0).astype(BF16)

    def pack(chosen, put):
        if bm:
            put(0, bm, chosen[0:bm, 0:half])
            put(bm, 2 * bm, chosen[0:bm, half:])
        if plan.block_tail:
            side = iota((2 * plan.block_tail, half), 0) // plan.block_tail
            value = jnp.where(side == 0, chosen[bm:, 0:half], chosen[bm:, half:])
            put(2 * bm, plan.block, value)

    per_block = plan.local * plan.capacity
    picked_rows = iota((ep_size * plan.picked, 1), 0)
    picked_slot = picked_rows // plan.picked
    codes = to_ep(picked_slot) * per_block + picked_code(
        plan, lax.rem(picked_rows, plan.picked)
    )
    chosen = jnp.dot(picks(codes.astype(F32), 0), normed, preferred_element_type=F32)
    for slot in range(ep_size):

        def put_out(first, last, value, slot=slot):
            out[slot, first:last] = value.astype(BF16)

        pack(chosen[slot * plan.picked : (slot + 1) * plan.picked], put_out)

    for copy in inputs[4:]:
        copy.wait()
    shard, width, heads = plan.shard, plan.width, plan.heads
    kv_ref[0:shard, 0:width] = key_ref[...]
    kv_ref[0:shard, width:] = value_ref[...]
    kv_ref[shard:] = jnp.zeros((kv_ref.shape[0] - shard, 2 * width), BF16)
    kv_ref[shard : shard + heads, 0:shard] = bias_ref[...]

    def info_copy(target, number, place):
        return send_of(info.at[0], info.at[target], info_sems, number, place)

    def go(slot):
        return send_of(
            out.at[slot], arrived.at[slot, 0], go_sems, slot, (to_ep(slot), own_tp)
        )

    def kv_line(source, step):
        return send_of(
            source, kv_all.at[2 * step], kv_line_sems, step, (own_ep + 2, own_tp)
        )

    def kv_pair(source, step):
        return send_of(source, kv_all.at[2 * step + 1], kv_pair_sems, step, to_pair)

    for target, place in ((1, to_across), (2, to_partner), (3, to_diagonal)):
        info_copy(target, target, place).start()
    go(1).start()

    def go_line(step):
        go(slot_to(step, 0)).start()
        go(slot_to(step, 1)).start()

    early = max(remote_lines - 1, 0)
    each(0, early, go_line)

    @pl.when(line + 1 < lines)
    def kv_first():
        kv_line(kv_ref, 1).start()

    each(early, remote_lines, go_line)

    @pl.when(parity == 0)
    def kv_to_pair():
        kv_pair(kv_ref, 0).start()

    head_of = iota((shard, width), 1) // plan.head_size
    queries = query_ref[...].astype(F32) * plan.head_size ** (-0.5)
    for head in range(heads):
        query_heads[head * shard : (head + 1) * shard] = jnp.where(
            head_of == head, queries, 0.0
        ).astype(BF16)
    attended[...] = jnp.zeros_like(attended)
    carried[...] = jnp.zeros_like(carried)

    def attend_block(load, own):
        keys = load(slice(0, shard), slice(0, width))
        values = load(slice(0, shard), slice(width, 2 * width))
        bias = load(slice(shard, shard + heads), slice(0, shard)).astype(F32)
        deep = (2 * shard, 2 * shard)
        row_key, column_key = lax.rem(iota(deep, 0), shard), iota(deep, 1)
        later_of = jnp.where((row_key > column_key) | (column_key >= shard), 1.0, 0.0)
        later_of = later_of.astype(BF16)
        before = iota((shard, shard), 1) < iota((shard, shard), 0)
        scores = lax.dot_general(
            query_heads[...], keys, (((1,), (1,)), ((), ())), preferred_element_type=F32
        )
        gained = attended[...]
        for head in range(heads):
            rows = slice(head * shard, (head + 1) * shard)
            score = scores[rows] + bias[head : head + 1]
            fails = -(jnp.maximum(score, 0.0) + jnp.log(1.0 + jnp.exp(-jnp.abs(score))))
            if own:
                hits = score + fails
                fails = jnp.where(before, fails, 0.0)
            else:
                hits = score + fails
            high = fails.astype(BF16)
            low = (fails - high.astype(F32)).astype(BF16)
            sums = jnp.dot(
                jnp.concatenate([high, low], axis=1), later_of, preferred_element_type=F32
            )
            taken = carried[rows]
            weights = jnp.exp(hits + sums[:, 0:shard] + taken)
            if own:
                weights = jnp.where(before, weights, 0.0)
            product = jnp.dot(weights.astype(BF16), values, preferred_element_type=F32)
            gained = gained + jnp.where(head_of == head, product, 0.0)
            carried[rows] = taken + sums[:, shard : 2 * shard]
        attended[...] = gained

    timed("attend_own", attend_block, lambda rows, cols: kv_ref[rows, cols], True)

    def attend_slot(slot):
        attend_block(lambda rows, cols: kv_all[slot, rows, cols], False)

    def kv_step(step):
        @pl.when(step <= line)
        def one():
            block = kv_all.at[2 * step]
            got("wait_kv_line", send_of(block, block, kv_line_sems, step, here))

            @pl.when(line + 1 < lines)
            def further():
                kv_line(block, step + 1).start()

            kv_pair(block, step).start()

    def attend_step(step):
        @pl.when(step <= line)
        def one():
            other = kv_all.at[2 * step + 1]
            got("wait_kv_pair", send_of(other, other, kv_pair_sems, step, here))

            def turn(side, c):
                timed("attend", attend_slot, 2 * step + lax.rem(side + 1 - parity, 2))
                return c

            lax.fori_loop(0, 2, turn, 0)

    def landed(slot):
        block = arrived.at[slot, 0]
        return send_of(block, block, go_sems, slot, here)

    def to_side(rel, slot, target, sems, place):
        return send_of(arrived.at[slot, rel], arrived.at[slot, target], sems, slot, place)

    got("wait_pair", landed(1))
    to_side(0, 1, 2, partner_sems, to_partner).start()

    got("wait_own_across", rows_over_x)
    own_all[1] = entry_norm(across_rows)
    own_copy(1, 3, 2, to_partner).start()
    info_copy(1, 1, here).wait_recv()

    def choose(target_ep, rel, put):
        place = iota((plan.picked, 1), 0)
        codes = target_ep * per_block + picked_code(plan, place)
        pack(
            jnp.dot(picks(codes.astype(F32), rel), own_all[rel], preferred_element_type=F32), put
        )

    def put_pair(first, last, value):
        out_pair[first:last] = value.astype(BF16)

    choose(pair_ep, 1, put_pair)
    pair_across = send_of(out_pair, arrived.at[1, 1], small_sems, PAIR_ACROSS, to_pair)
    pair_across.start()

    def forward_side(step, side):
        slot = slot_of(step, side)
        got("wait_landed", landed(slot))
        to_side(0, slot, 1, across_sems, to_across).start()
        to_side(0, slot, 2, partner_sems, to_partner).start()

    def forward(step):
        for side in range(2):
            forward_side(step, side)

    if remote_lines:
        forward_side(0, 0)

    def relay(step, side):
        slot = slot_of(step, side)
        got("wait_across", to_side(1, slot, 1, across_sems, here))
        to_side(1, slot, 3, relay_sems, to_partner).start()

    got("wait_own_partner", own_copy(2, 2, 1, here))
    got("wait_own_diag", own_copy(3, 3, 2, here))
    for rel in (2, 3):
        info_copy(rel, rel, here).wait_recv()
    for rel in range(tp_size):
        info_cols[rel, :, 0:8] = turned(info[rel])
    for copy in weights[0:3]:
        copy.wait()

    def shared_expert():
        shared_rows = own_all[...].reshape(tp_size * rows_n, plan.model)
        hidden = silu(jnp.dot(shared_rows, shared_gate_w[...], preferred_element_type=F32))
        hidden = hidden * jnp.dot(shared_rows, shared_up_w[...], preferred_element_type=F32)
        shared_acc[...] = jnp.dot(
            hidden.astype(BF16), shared_down_w[...], preferred_element_type=F32
        ).reshape(shared_acc.shape)

    timed("shared", shared_expert)
    if remote_lines:
        forward_side(0, 1)

    def put_own(first, last, value, rel):
        arrived[0, rel, first:last] = value.astype(BF16)

    def choose_own():
        arrived[0, 0] = out[0]
        for rel in (1, 2, 3):
            choose(own_ep, rel, functools.partial(put_own, rel=rel))

    timed("choose_own", choose_own)

    blocks = 2 * tp_size
    tails = blocks * plan.tail
    folded = blocks * 2 * plan.block_tail

    def tail_move(side, by_column):
        shape = (folded, plan.local * tails) if by_column else (plan.local * tails, folded)
        sorted_at = iota(shape, 1 if by_column else 0)
        folded_at = iota(shape, 0 if by_column else 1)
        expert = sorted_at // tails
        block = lax.rem(sorted_at, tails) // plan.tail
        spot = lax.rem(sorted_at, plan.tail)
        target = (
            block * 2 * plan.block_tail + side * plan.block_tail + expert * plan.tail + spot
        )
        return jnp.where(folded_at == target, 1.0, 0.0).astype(BF16)

    def experts(first):
        pair = arrived.at[pl.ds(first, 2)]
        tail_rows = None
        if plan.tail:
            folded_rows = pair[:, :, 2 * bm : plan.block].reshape(folded, half)
            tail_rows = jnp.concatenate(
                [
                    jnp.dot(tail_move(side, False), folded_rows, preferred_element_type=F32)
                    for side in range(2)
                ],
                axis=1,
            ).astype(BF16)
        tail_results = []
        for expert in range(plan.local):
            pieces = []
            if plan.main:
                at = expert * plan.main
                left = pair[:, :, at : at + plan.main]
                right = pair[:, :, bm + at : bm + at + plan.main]
                pieces.append(
                    jnp.concatenate([left, right], axis=3).reshape(
                        blocks * plan.main, plan.model
                    )
                )
            if plan.tail:
                pieces.append(tail_rows[expert * tails : (expert + 1) * tails])
            x = pieces[0] if len(pieces) == 1 else jnp.concatenate(pieces, axis=0)
            hidden = silu(jnp.dot(x, gate_w[expert], preferred_element_type=F32))
            hidden = hidden * jnp.dot(x, up_w[expert], preferred_element_type=F32)
            result_rows = jnp.dot(
                hidden.astype(BF16), down_w[expert], preferred_element_type=F32
            ).astype(BF16)
            if plan.main:
                at = expert * plan.main
                shape = (2, tp_size, plan.main, half)
                count = blocks * plan.main
                part[pl.ds(first, 2), :, at : at + plan.main] = result_rows[
                    0:count, 0:half
                ].reshape(shape)
                part[pl.ds(first, 2), :, bm + at : bm + at + plan.main] = result_rows[
                    0:count, half:
                ].reshape(shape)
            if plan.tail:
                tail_results.append(result_rows[blocks * plan.main :])
        if plan.tail:
            ends = jnp.concatenate(tail_results, axis=0)
            value = jnp.dot(
                tail_move(0, True), ends[:, 0:half], preferred_element_type=F32
            ) + jnp.dot(tail_move(1, True), ends[:, half:], preferred_element_type=F32)
            part[pl.ds(first, 2), :, 2 * bm : plan.block] = value.astype(BF16).reshape(
                2, tp_size, 2 * plan.block_tail, half
            )

    def mixed(target_ep, rel, load):
        place = iota((1, plan.block), 1)
        code, side = block_code(plan, place)
        code = (code + target_ep * per_block).astype(F32)
        weight = jnp.zeros((rows_n, plan.block), F32)
        for k in range(plan.top):
            hit = code == info_cols[rel, 0:rows_n, k : k + 1]
            at = plan.top + k
            weight = weight + jnp.where(hit, info_cols[rel, 0:rows_n, at : at + 1], 0.0)
        sums = []
        for which in range(2):
            kept = jnp.where(side == which, weight, 0.0)
            high = kept.astype(BF16)
            low = (kept - high.astype(F32)).astype(BF16)
            value = jnp.dot(
                jnp.concatenate([high, low], axis=0), load(), preferred_element_type=F32
            )
            sums.append(value[0:rows_n] + value[rows_n:])
        return jnp.concatenate(sums, axis=1)

    def near(slot):
        return send_of(
            part.at[slot, pl.ds(2, 2)], near_in.at[slot], near_sems, slot, to_partner
        )

    block = arrived.at[1, 1]
    got("wait_pair_across", send_of(block, block, small_sems, PAIR_ACROSS, here))
    to_side(1, 1, 3, relay_sems, to_partner).start()
    got("wait_pair_p", to_side(2, 1, 2, partner_sems, here))
    got("wait_pair_r", to_side(3, 1, 3, relay_sems, here))
    for copy in weights[3:6]:
        copy.wait()
    timed("experts_own", experts, 0)
    near(1).start()
    if remote_lines > 1:
        forward(1)

    def fold_own():
        for rel in range(tp_size):
            shared_acc[rel] = shared_acc[rel] + mixed(own_ep, rel, lambda rel=rel: part[0, rel])

    timed("fold_own", fold_own)
    if remote_lines:
        relay(0, 0)
    shared_near[...] = shared_acc[2:4].astype(BF16)
    shared_near_copy = send_of(shared_near, near_shared, small_sems, NEAR_SHARED, to_partner)
    shared_near_copy.start()
    got("wait_near1", near(1))
    pair_out[...] = (part[1, 0:2].astype(F32) + near_in[1].astype(F32)).astype(BF16)
    pair_back = send_of(pair_out, pair_in, small_sems, PAIR_BACK, to_pair)
    pair_back.start()

    @pl.when(parity == 1)
    def attend_pair():
        block = kv_all.at[1]
        got("wait_kv_pair", send_of(block, block, kv_pair_sems, 0, here))
        timed("attend", attend_slot, 1)

    if remote_lines:
        kv_step(1)


    def ready(step):
        for side in range(2):
            slot = slot_of(step, side)
            got("wait_partner", to_side(2, slot, 2, partner_sems, here))
            got("wait_relay", to_side(3, slot, 3, relay_sems, here))

    def far(slot):
        return send_of(far_out.at[slot], far_in.at[slot], far_sems, slot, to_across)

    def twin_copy(side):
        return send_of(
            twin_out.at[side],
            twin_in.at[side],
            small_sems,
            TWIN + side,
            (from_ep(twin_from + side), own_tp),
        )

    def send_far(step):
        is_twin = (other_line(step) == twin) & outer
        for side in range(2):
            slot = slot_of(step, side)
            got("wait_near", near(slot))

            def over_x(slot=slot):
                value = part[slot, 1].astype(F32) + near_in[slot, 1].astype(F32)
                far_out[slot] = value.astype(BF16)
                far(slot).start()

            def straight(slot=slot, side=side):
                value = part[slot, 0:2].astype(F32) + near_in[slot].astype(F32)
                twin_out[side] = value.astype(BF16)
                twin_copy(side).start()

            if side in STRAIGHT:
                pl.when(is_twin)(straight)
                pl.when(jnp.logical_not(is_twin))(over_x)
            else:
                over_x()

    def give_back(slot):
        return send_of(
            total.at[slot], back.at[slot], return_sems, slot, (from_ep(slot), own_tp)
        )

    def send_total(step):
        def reduced(slot):
            got("wait_far", far(slot))
            total[slot] = (
                part[slot, 0].astype(F32)
                + near_in[slot, 0].astype(F32)
                + far_in[slot].astype(F32)
            ).astype(BF16)
            give_back(slot).start()

        for side in range(2):
            if side in STRAIGHT:
                pl.when((other_line(step) != twin) | inner)(
                    functools.partial(reduced, slot_of(step, side))
                )
            else:
                reduced(slot_of(step, side))

    def turn(step):
        @pl.when(step >= 2)
        def relay_first():
            relay(step - 1, 0)

        relay(step - 1, 1)

        @pl.when(step >= 3)
        def attend_line():
            attend_step(step - 2)

        ready(step - 1)
        timed("experts", experts, slot_of(step - 1, 0))
        for side in range(2):
            near(slot_of(step - 1, side)).start()

        send_far(step - 1)

        @pl.when(step + 1 < remote_lines)
        def next_line():
            forward(step + 1)

        kv_step(step + 1)

        @pl.when(step >= 2)
        def answer():
            send_total(step - 2)

    if remote_lines:
        each(1, remote_lines + 1, turn)

    def folded_rows(rel):
        value = shared_acc[rel] + near_shared[rel].astype(F32)
        return value + mixed(pair_ep, rel, lambda: pair_in[rel])

    def fold_twin(rel):
        value = result[...]
        for side in STRAIGHT:
            value = value + mixed(
                to_ep(twin_to + side), rel, lambda side=side: twin_in[side, rel]
            )
        result[...] = value

    got("wait_near_shared", shared_near_copy)
    got("wait_pair_back", pair_back)
    result[...] = folded_rows(1)
    if remote_lines:

        @pl.when(inner)
        def with_twin():
            for side in STRAIGHT:
                got("wait_twin", twin_copy(side))
            fold_twin(1)

    far_shared_out[...] = result[...].astype(BF16)
    shared_far_copy = send_of(far_shared_out, far_shared, small_sems, FAR_SHARED, to_across)
    shared_far_copy.start()
    each(max(remote_lines - 1, 1), remote_lines + 1, attend_step)
    weights[6].wait()
    rows_out = shard // tp_size
    mixer_term = jnp.dot(
        attended[...].astype(BF16), mixer_w[...], preferred_element_type=F32
    ).astype(BF16)
    for place in range(tp_size):
        high = lax.rem(place // 2 + own_tp // 2, 2)
        low = lax.rem(place + own_tp, 2)
        mix_part[high + 2 * low] = mixer_term[place * rows_out : (place + 1) * rows_out]
    mix_near_copy = send_of(
        mix_part.at[pl.ds(2, 2)], near_mix, small_sems, NEAR_MIX, to_partner
    )
    mix_near_copy.start()
    if remote_lines:
        send_total(remote_lines - 1)
    got("wait_near_mix", mix_near_copy)
    far_mix_out[...] = (mix_part[1].astype(F32) + near_mix[1].astype(F32)).astype(BF16)
    mix_far_copy = send_of(far_mix_out, far_mix, small_sems, FAR_MIX, to_across)
    mix_far_copy.start()
    result[...] = folded_rows(0)
    if remote_lines:
        pl.when(inner)(functools.partial(fold_twin, 0))

    rows_over_x.wait_send()
    own_copy(0, 2, 1, to_partner).wait_send()
    own_copy(1, 3, 2, to_partner).wait_send()
    for target, place in ((1, to_across), (2, to_partner), (3, to_diagonal)):
        info_copy(target, target, place).wait_send()
    go(1).wait_send()
    to_side(0, 1, 2, partner_sems, to_partner).wait_send()
    to_side(1, 1, 3, relay_sems, to_partner).wait_send()
    near(1).wait_send()
    for copy in (pair_across, pair_back, shared_near_copy, mix_near_copy):
        copy.wait_send()

    def is_straight(slot):
        found = slot < 0
        for side in STRAIGHT:
            found = found | ((slot == twin_from + side) & outer)
        return found

    def finish(slot):
        go(slot).wait_send()
        to_side(0, slot, 1, across_sems, to_across).wait_send()
        to_side(0, slot, 2, partner_sems, to_partner).wait_send()
        to_side(1, slot, 3, relay_sems, to_partner).wait_send()
        near(slot).wait_send()

        @pl.when(jnp.logical_not(is_straight(slot)))
        def reduced():
            far(slot).wait_send()

    each(2, ep_size, finish)

    if remote_lines:

        @pl.when(outer)
        def sent_twin():
            for side in STRAIGHT:
                twin_copy(side).wait_send()

    def finish_kv(step):
        @pl.when((step <= line) & (line + 1 < lines))
        def sent_on():
            kv_line(kv_all.at[2 * step], step + 1).wait_send()

        @pl.when((step <= line) & (step >= 1))
        def sent_over():
            kv_pair(kv_all.at[2 * step], step).wait_send()

    each(0, lines, finish_kv)

    @pl.when(parity == 0)
    def sent_pair():
        kv_pair(kv_ref, 0).wait_send()

    def take_back(step):
        def one(slot):
            block = back.at[slot]
            got("wait_back", send_of(block, block, return_sems, slot, here))
            result[...] = result[...] + mixed(to_ep(slot), 0, lambda: back[slot])

        for side in range(2):
            if side in STRAIGHT:
                pl.when((other_line(step) != twin) | outer)(
                    functools.partial(one, slot_to(step, side))
                )
            else:
                one(slot_to(step, side))

    each(0, remote_lines, take_back)

    def returned(slot):
        @pl.when(jnp.logical_not(is_straight(slot)))
        def one():
            give_back(slot).wait_send()

    timed("drain_returns", each, 2, ep_size, returned)
    got("wait_far_shared", shared_far_copy)
    with jax.named_scope("final_expert"):
        combined = result[...] + far_shared[...].astype(F32)
        expert_out[...] = root_norm(combined, exit_ref[...]).astype(BF16)
    expert_write = pltpu.make_async_copy(expert_out, expert_hbm_out, output_sem.at[0])
    expert_write.start()
    got("wait_far_mix", mix_far_copy)
    with jax.named_scope("final_mixer"):
        mixer_sum = mix_part[0].astype(F32) + near_mix[0].astype(F32) + far_mix[...].astype(F32)
        mixer_out[...] = root_norm(mixer_sum, mixer_gain_ref[...]).astype(BF16)
    mixer_write = pltpu.make_async_copy(mixer_out, mixer_hbm_out, output_sem.at[1])
    mixer_write.start()
    shared_far_copy.wait_send()
    mix_far_copy.wait_send()
    with jax.named_scope("writes"):
        expert_write.wait()
        mixer_write.wait()


def hand_on(mixer_in, expert_in, mixer_out, expert_out, mixer_held, expert_held, sems):
    arrays = [(expert_in, expert_held, expert_out), (mixer_in, mixer_held, mixer_out)]
    reads = [
        pltpu.make_async_copy(source, held, sems.at[0, number])
        for number, (source, held, target) in enumerate(arrays)
    ]
    writes = [
        pltpu.make_async_copy(held, target, sems.at[1, number])
        for number, (source, held, target) in enumerate(arrays)
    ]
    for read in reads:
        read.start()
    for read, write in zip(reads, writes):
        read.wait()
        write.start()
    for write in writes:
        write.wait()


def on_device(
    query_rows,
    key_rows,
    value_rows,
    key_bias,
    mixer_weight,
    mixer_gain,
    routed_input,
    entry_gain,
    expert_index,
    route_weights,
    expert_gate,
    expert_up,
    expert_down,
    shared_gate,
    shared_up,
    shared_down,
    exit_gain,
):
    ep_size = lax.axis_size("ep")
    tp_size = lax.axis_size("tp")
    plan = Plan(
        ep_size, tp_size, key_bias.shape[1], query_rows, routed_input, expert_index, expert_gate
    )
    shard, width, model, rows = plan.shard, plan.width, plan.model, plan.rows
    kv_rows = shard + -(-plan.heads // 8) * 8
    small = [
        routed_input,
        entry_gain.reshape(1, model),
        jnp.transpose(expert_index),
        jnp.transpose(route_weights),
        key_rows,
        value_rows,
        jnp.transpose(key_bias),
        query_rows,
        exit_gain.reshape(1, model),
        mixer_gain.reshape(1, model),
    ]
    large = [
        mixer_weight,
        expert_gate,
        expert_up,
        expert_down,
        shared_gate,
        shared_up,
        shared_down,
    ]
    block = (plan.block, plan.half)
    mix = (shard // tp_size, model)

    def buffer(*shape, kind=BF16):
        return pltpu.VMEM(shape, kind)

    sem = pltpu.SemaphoreType.DMA
    hbm = pl.BlockSpec(memory_space=pltpu.HBM)
    scratch = [buffer(*mix), buffer(rows, model), sem((2,))]
    scratch += [pltpu.VMEM(value.shape, value.dtype) for value in small + large]
    scratch += [
        buffer(rows, model),
        buffer(tp_size, rows, model),
        buffer(tp_size, 8, plan.padded_rows, kind=F32),
        buffer(tp_size, plan.padded_rows, 128, kind=F32),
        buffer(ep_size, *block),
        buffer(*block),
        buffer(ep_size, tp_size, *block),
        buffer(ep_size, tp_size, *block),
        buffer(ep_size, 2, *block),
        buffer(ep_size, *block),
        buffer(ep_size, *block),
        buffer(ep_size, *block),
        buffer(ep_size, *block),
        buffer(2, *block),
        buffer(2, *block),
        buffer(2, 2, *block),
        buffer(2, 2, *block),
        buffer(tp_size, rows, model, kind=F32),
        buffer(2, rows, model),
        buffer(2, rows, model),
        buffer(rows, model),
        buffer(rows, model),
        buffer(rows, model, kind=F32),
        buffer(tp_size, *mix),
        buffer(2, *mix),
        buffer(*mix),
        buffer(*mix),
        buffer(kv_rows, 2 * width),
        buffer(ep_size, kv_rows, 2 * width),
        buffer(plan.heads * shard, width),
        buffer(plan.heads * shard, shard, kind=F32),
        buffer(shard, width, kind=F32),
    ]
    scratch += [sem((len(small),)), sem((len(large),))]
    for count in (4, 4, ep_size, ep_size, ep_size, ep_size, ep_size, ep_size, ep_size, ep_size, ep_size, 8):
        scratch += [sem((count,)), sem((count,))]
    results = pl.pallas_call(
        functools.partial(layer_kernel, plan),
        out_shape=(
            jax.ShapeDtypeStruct(mix, BF16),
            jax.ShapeDtypeStruct((rows, model), BF16),
        ),
        in_specs=[hbm] * len(small + large),
        out_specs=(hbm, hbm),
        scratch_shapes=scratch,
        compiler_params=pltpu.CompilerParams(
            collective_id=0, has_side_effects=True, vmem_limit_bytes=62 * 1024 * 1024
        ),
        name="whole_layer",
    )(*small, *large)
    return pl.pallas_call(
        hand_on,
        out_shape=(
            jax.ShapeDtypeStruct(mix, BF16),
            jax.ShapeDtypeStruct((rows, model), BF16),
        ),
        in_specs=[hbm] * 2,
        out_specs=(hbm, hbm),
        scratch_shapes=[buffer(*mix), buffer(rows, model), sem((2, 2))],
        name="hand_on",
    )(*results)


def solution(mesh):
    in_specs = (
        P("ep", "tp"),
        P("ep", "tp"),
        P("ep", "tp"),
        P("ep", "tp"),
        P("tp", None),
        P(),
        P(("ep", "tp"), None),
        P(),
        P(("ep", "tp"), None),
        P(("ep", "tp"), None),
        P("ep", None, "tp"),
        P("ep", None, "tp"),
        P("ep", "tp", None),
        P(None, "tp"),
        P(None, "tp"),
        P("tp", None),
        P(),
    )
    out_specs = (P(("ep", "tp"), None), P(("ep", "tp"), None))
    return jax.shard_map(
        on_device, mesh=mesh, in_specs=in_specs, out_specs=out_specs, check_vma=False
    )
```

```python
import functools

import jax
import jax.numpy as jnp
from jax import lax
from jax.experimental import pallas as pl
from jax.experimental.pallas import tpu as pltpu
from jax.sharding import PartitionSpec as P

MESH = pl.DeviceIdType.MESH
EPS = 1e-06
F32 = jnp.float32
BF16 = jnp.bfloat16
STRAIGHT = (0,)


class Plan:
    def __init__(self, ep_size, tp_size, head_count, query, rows, index, gate):
        self.ep = ep_size
        self.tp = tp_size
        self.lines = ep_size // 2
        self.heads = head_count
        self.shard, self.width = query.shape
        self.head_size = self.width // head_count
        self.rows, self.model = rows.shape
        self.half = self.model // 2
        self.top = index.shape[1]
        self.local = gate.shape[0]
        self.hidden = gate.shape[2]
        self.experts = self.local * ep_size
        self.capacity = 3 * self.rows * self.top // (2 * self.experts)
        self.main = self.capacity // 16 * 16
        self.tail = self.capacity - self.main
        self.block_main = self.local * self.main
        self.block_tail = self.local * self.tail
        self.picked = self.block_main + 2 * self.block_tail
        self.block = 2 * self.block_main + 2 * self.block_tail
        self.named = -(-self.experts // 16) * 16
        self.padded_rows = -(-self.rows // 128) * 128


def send_of(source, target, sems, slot, place):
    return pltpu.make_async_remote_copy(
        src_ref=source,
        dst_ref=target,
        send_sem=sems[0].at[slot],
        recv_sem=sems[1].at[slot],
        device_id=place,
        device_id_type=MESH,
    )


def got(name, copy):
    with jax.named_scope(name):
        copy.wait_recv()


def timed(name, action, *args):
    with jax.named_scope(name):
        return action(*args)


def iota(shape, axis):
    return lax.broadcasted_iota(jnp.int32, shape, axis)


def root_norm(values, gain_row):
    return values * lax.rsqrt(jnp.mean(values * values, axis=-1, keepdims=True) + EPS) * gain_row


def silu(value):
    return value / (1.0 + jnp.exp(-value))


def tail_code(plan, place):
    row = lax.rem(place, plan.block_tail)
    return row // plan.tail * plan.capacity + plan.main + lax.rem(row, plan.tail)


def picked_code(plan, place):
    if plan.main == 0:
        return tail_code(plan, place)
    code = place // plan.main * plan.capacity + lax.rem(place, plan.main)
    if plan.tail == 0:
        return code
    after = jnp.maximum(place - plan.block_main, 0)
    return jnp.where(place < plan.block_main, code, tail_code(plan, after))


def block_code(plan, place):
    bm = plan.block_main
    if bm == 0:
        return tail_code(plan, place), place // plan.block_tail
    row = lax.rem(place, bm)
    code = row // plan.main * plan.capacity + lax.rem(row, plan.main)
    side = place // bm
    if plan.tail == 0:
        return code, side
    after = jnp.maximum(place - 2 * bm, 0)
    is_tail = place >= 2 * bm
    return (
        jnp.where(is_tail, tail_code(plan, after), code),
        jnp.where(is_tail, after // plan.block_tail, side),
    )


def layer_kernel(plan, *refs):
    (
        input_hbm,
        entry_hbm,
        index_hbm,
        route_hbm,
        key_hbm,
        value_hbm,
        bias_hbm,
        query_hbm,
        exit_hbm,
        mixer_gain_hbm,
        mixer_hbm,
        gate_hbm,
        up_hbm,
        down_hbm,
        shared_gate_hbm,
        shared_up_hbm,
        shared_down_hbm,
        mixer_hbm_out,
        expert_hbm_out,
        mixer_out,
        expert_out,
        output_sem,
        input_ref,
        entry_ref,
        index_ref,
        route_ref,
        key_ref,
        value_ref,
        bias_ref,
        query_ref,
        exit_ref,
        mixer_gain_ref,
        mixer_w,
        gate_w,
        up_w,
        down_w,
        shared_gate_w,
        shared_up_w,
        shared_down_w,
        across_rows,
        own_all,
        info,
        info_cols,
        out,
        out_pair,
        arrived,
        part,
        near_in,
        far_out,
        far_in,
        total,
        back,
        pair_out,
        pair_in,
        twin_out,
        twin_in,
        shared_acc,
        shared_near,
        near_shared,
        far_shared_out,
        far_shared,
        result,
        mix_part,
        near_mix,
        far_mix_out,
        far_mix,
        kv_ref,
        kv_all,
        query_heads,
        carried,
        attended,
        input_sem,
        weight_sem,
        own_send,
        own_recv,
        info_send,
        info_recv,
        kv_line_send,
        kv_line_recv,
        kv_pair_send,
        kv_pair_recv,
        go_send,
        go_recv,
        across_send,
        across_recv,
        partner_send,
        partner_recv,
        relay_send,
        relay_recv,
        near_send,
        near_recv,
        far_send,
        far_recv,
        return_send,
        return_recv,
        small_send,
        small_recv,
    ) = refs
    ep_size, tp_size, lines = plan.ep, plan.tp, plan.lines
    rows_n, half = plan.rows, plan.half
    bm = plan.block_main
    own_ep = lax.axis_index("ep")
    own_tp = lax.axis_index("tp")
    partner_tp = own_tp + 1 - 2 * lax.rem(own_tp, 2)
    across_tp = lax.rem(own_tp + tp_size // 2, tp_size)
    diagonal_tp = lax.rem(partner_tp + tp_size // 2, tp_size)
    line = own_ep // 2
    parity = lax.rem(own_ep, 2)
    pair_ep = own_ep + 1 - 2 * parity
    to_across = (own_ep, across_tp)
    to_partner = (own_ep, partner_tp)
    to_diagonal = (own_ep, diagonal_tp)
    to_pair = (pair_ep, own_tp)
    here = (own_ep, own_tp)

    own_sems = (own_send, own_recv)
    info_sems = (info_send, info_recv)
    kv_line_sems = (kv_line_send, kv_line_recv)
    kv_pair_sems = (kv_pair_send, kv_pair_recv)
    go_sems = (go_send, go_recv)
    across_sems = (across_send, across_recv)
    partner_sems = (partner_send, partner_recv)
    relay_sems = (relay_send, relay_recv)
    near_sems = (near_send, near_recv)
    far_sems = (far_send, far_recv)
    return_sems = (return_send, return_recv)
    small_sems = (small_send, small_recv)
    PAIR_ACROSS, PAIR_BACK, NEAR_SHARED, FAR_SHARED, NEAR_MIX, FAR_MIX, TWIN = range(7)

    def to_ep(slot):
        return 2 * lax.rem(line + slot // 2, lines) + lax.rem(parity + slot, 2)

    def from_ep(slot):
        return 2 * lax.rem(line - slot // 2 + lines, lines) + lax.rem(parity + slot, 2)

    def each(first, last, action):
        lax.fori_loop(first, last, lambda step, c: (action(step), c)[1], 0)

    remote_lines = lines - 1

    def other_line(step):
        middle = lines // 2
        margin = jnp.minimum(line, lines - 1 - line)
        index = jnp.where(step <= middle + margin - 1, step - 1, step)
        around = index < 2 * margin
        distance = jnp.where(around, index // 2 + 1, index - margin + 1)
        to_end = jnp.where(around, lax.rem(index, 2), 1)
        upward = (2 * line < lines) == (to_end == 1)
        near_line = jnp.where(upward, line + distance, line - distance)
        return jnp.where(step == 0, lax.rem(line + middle, lines), near_line)

    twin = line + 1 - 2 * lax.rem(line, 2)
    twin_from = 2 * lax.rem(line - twin + lines, lines)
    twin_to = 2 * lax.rem(twin - line + lines, lines)
    outer = (lax.rem(line, 2) == 0) == (2 * line < lines)
    inner = jnp.logical_not(outer)

    def slot_of(step, side):
        return 2 * lax.rem(line - other_line(step) + lines, lines) + side

    def slot_to(step, side):
        return 2 * lax.rem(other_line(step) - line + lines, lines) + side

    barrier = pltpu.get_barrier_semaphore()

    def greet(step):
        place = lax.rem(own_ep + step, ep_size)
        pl.semaphore_signal(barrier, inc=1, device_id=(place, own_tp), device_id_type=MESH)

    each(1, ep_size, greet)
    for place in (partner_tp, across_tp, diagonal_tp):
        pl.semaphore_signal(barrier, inc=1, device_id=(own_ep, place), device_id_type=MESH)

    inputs = [
        pltpu.make_async_copy(source, target, input_sem.at[number])
        for number, (source, target) in enumerate(
            [
                (input_hbm, input_ref),
                (entry_hbm, entry_ref),
                (index_hbm, index_ref),
                (route_hbm, route_ref),
                (key_hbm, key_ref),
                (value_hbm, value_ref),
                (bias_hbm, bias_ref),
                (query_hbm, query_ref),
                (exit_hbm, exit_ref),
                (mixer_gain_hbm, mixer_gain_ref),
            ]
        )
    ]
    for copy in inputs:
        copy.start()

    weights = [
        pltpu.make_async_copy(source, target, weight_sem.at[number])
        for number, (source, target) in enumerate(
            [
                (shared_gate_hbm, shared_gate_w),
                (shared_up_hbm, shared_up_w),
                (shared_down_hbm, shared_down_w),
                (gate_hbm, gate_w),
                (up_hbm, up_w),
                (down_hbm, down_w),
                (mixer_hbm, mixer_w),
            ]
        )
    ]
    for copy in weights:
        copy.start()

    inputs[0].wait()
    with jax.named_scope("wait_barrier"):
        pl.semaphore_wait(barrier, ep_size - 1 + 3)

    def own_copy(source, target, number, place):
        return send_of(own_all.at[source], own_all.at[target], own_sems, number, place)

    rows_over_x = send_of(input_ref, across_rows, own_sems, 0, to_across)
    rows_over_x.start()

    def entry_norm(ref):
        return root_norm(ref[...].astype(F32), entry_ref[...]).astype(BF16)

    for copy in inputs[1:4]:
        copy.wait()
    normed = entry_norm(input_ref)
    own_all[0] = normed
    own_copy(0, 2, 1, to_partner).start()

    expert_at = iota((plan.named, rows_n), 0)
    named = [expert_at == index_ref[k : k + 1] for k in range(plan.top)]
    both = jnp.zeros((plan.named, rows_n), F32)
    for one in named:
        both = both + jnp.where(one, 1.0, 0.0)
    earlier = jnp.where(iota((rows_n, rows_n), 0) < iota((rows_n, rows_n), 1), 1.0, 0.0)
    rank = jnp.dot(both.astype(BF16), earlier.astype(BF16), preferred_element_type=F32)
    rank = rank + expert_at.astype(F32) * plan.capacity
    info[0] = jnp.zeros_like(info[0])
    for k, one in enumerate(named):
        code = jnp.sum(jnp.where(one, rank, 0.0), axis=0, keepdims=True)
        info[0, k : k + 1, 0:rows_n] = code
        info[0, plan.top + k : plan.top + k + 1, 0:rows_n] = route_ref[k : k + 1]

    def turned(value):
        return jnp.transpose(value, (1, 0))

    def picks(codes, rel):
        hit = codes == info[rel, 0:1, 0:rows_n]
        for k in range(1, plan.top):
            hit = hit | (codes == info[rel, k : k + 1, 0:rows_n])
        return jnp.where(hit, 1.0, 0.0).astype(BF16)

    def pack(chosen, put):
        if bm:
            put(0, bm, chosen[0:bm, 0:half])
            put(bm, 2 * bm, chosen[0:bm, half:])
        if plan.block_tail:
            side = iota((2 * plan.block_tail, half), 0) // plan.block_tail
            value = jnp.where(side == 0, chosen[bm:, 0:half], chosen[bm:, half:])
            put(2 * bm, plan.block, value)

    per_block = plan.local * plan.capacity
    picked_rows = iota((ep_size * plan.picked, 1), 0)
    picked_slot = picked_rows // plan.picked
    codes = to_ep(picked_slot) * per_block + picked_code(
        plan, lax.rem(picked_rows, plan.picked)
    )
    chosen = jnp.dot(picks(codes.astype(F32), 0), normed, preferred_element_type=F32)
    for slot in range(ep_size):

        def put_out(first, last, value, slot=slot):
            out[slot, first:last] = value.astype(BF16)

        pack(chosen[slot * plan.picked : (slot + 1) * plan.picked], put_out)

    for copy in inputs[4:]:
        copy.wait()
    shard, width, heads = plan.shard, plan.width, plan.heads
    kv_ref[0:shard, 0:width] = key_ref[...]
    kv_ref[0:shard, width:] = value_ref[...]
    kv_ref[shard:] = jnp.zeros((kv_ref.shape[0] - shard, 2 * width), BF16)
    kv_ref[shard : shard + heads, 0:shard] = bias_ref[...]

    def info_copy(target, number, place):
        return send_of(info.at[0], info.at[target], info_sems, number, place)

    def go(slot):
        return send_of(
            out.at[slot], arrived.at[slot, 0], go_sems, slot, (to_ep(slot), own_tp)
        )

    def kv_line(source, step):
        return send_of(
            source, kv_all.at[2 * step], kv_line_sems, step, (own_ep + 2, own_tp)
        )

    def kv_pair(source, step):
        return send_of(source, kv_all.at[2 * step + 1], kv_pair_sems, step, to_pair)

    for target, place in ((1, to_across), (2, to_partner), (3, to_diagonal)):
        info_copy(target, target, place).start()
    go(1).start()

    def go_line(step):
        go(slot_to(step, 0)).start()
        go(slot_to(step, 1)).start()

    early = max(remote_lines - 1, 0)
    each(0, early, go_line)

    @pl.when(line + 1 < lines)
    def kv_first():
        kv_line(kv_ref, 1).start()

    each(early, remote_lines, go_line)

    @pl.when(parity == 0)
    def kv_to_pair():
        kv_pair(kv_ref, 0).start()

    head_of = iota((shard, width), 1) // plan.head_size
    queries = query_ref[...].astype(F32) * plan.head_size ** (-0.5)
    for head in range(heads):
        query_heads[head * shard : (head + 1) * shard] = jnp.where(
            head_of == head, queries, 0.0
        ).astype(BF16)
    attended[...] = jnp.zeros_like(attended)
    carried[...] = jnp.zeros_like(carried)

    def attend_block(load, own):
        keys = load(slice(0, shard), slice(0, width))
        values = load(slice(0, shard), slice(width, 2 * width))
        bias = load(slice(shard, shard + heads), slice(0, shard)).astype(F32)
        deep = (2 * shard, 2 * shard)
        row_key, column_key = lax.rem(iota(deep, 0), shard), iota(deep, 1)
        later_of = jnp.where((row_key > column_key) | (column_key >= shard), 1.0, 0.0)
        later_of = later_of.astype(BF16)
        before = iota((shard, shard), 1) < iota((shard, shard), 0)
        scores = lax.dot_general(
            query_heads[...], keys, (((1,), (1,)), ((), ())), preferred_element_type=F32
        )
        gained = attended[...]
        for head in range(heads):
            rows = slice(head * shard, (head + 1) * shard)
            score = scores[rows] + bias[head : head + 1]
            fails = -(jnp.maximum(score, 0.0) + jnp.log(1.0 + jnp.exp(-jnp.abs(score))))
            if own:
                hits = score + fails
                fails = jnp.where(before, fails, 0.0)
            else:
                hits = score + fails
            high = fails.astype(BF16)
            low = (fails - high.astype(F32)).astype(BF16)
            sums = jnp.dot(
                jnp.concatenate([high, low], axis=1), later_of, preferred_element_type=F32
            )
            taken = carried[rows]
            weights = jnp.exp(hits + sums[:, 0:shard] + taken)
            if own:
                weights = jnp.where(before, weights, 0.0)
            product = jnp.dot(weights.astype(BF16), values, preferred_element_type=F32)
            gained = gained + jnp.where(head_of == head, product, 0.0)
            carried[rows] = taken + sums[:, shard : 2 * shard]
        attended[...] = gained

    timed("attend_own", attend_block, lambda rows, cols: kv_ref[rows, cols], True)

    def attend_slot(slot):
        attend_block(lambda rows, cols: kv_all[slot, rows, cols], False)

    def kv_step(step):
        @pl.when(step <= line)
        def one():
            block = kv_all.at[2 * step]
            got("wait_kv_line", send_of(block, block, kv_line_sems, step, here))

            @pl.when(line + 1 < lines)
            def further():
                kv_line(block, step + 1).start()

            kv_pair(block, step).start()

    def attend_step(step):
        @pl.when(step <= line)
        def one():
            other = kv_all.at[2 * step + 1]
            got("wait_kv_pair", send_of(other, other, kv_pair_sems, step, here))

            def turn(side, c):
                timed("attend", attend_slot, 2 * step + lax.rem(side + 1 - parity, 2))
                return c

            lax.fori_loop(0, 2, turn, 0)

    def landed(slot):
        block = arrived.at[slot, 0]
        return send_of(block, block, go_sems, slot, here)

    def to_side(rel, slot, target, sems, place):
        return send_of(arrived.at[slot, rel], arrived.at[slot, target], sems, slot, place)

    got("wait_pair", landed(1))
    to_side(0, 1, 2, partner_sems, to_partner).start()

    got("wait_own_across", rows_over_x)
    own_all[1] = entry_norm(across_rows)
    own_copy(1, 3, 2, to_partner).start()
    info_copy(1, 1, here).wait_recv()

    def choose(target_ep, rel, put):
        place = iota((plan.picked, 1), 0)
        codes = target_ep * per_block + picked_code(plan, place)
        pack(
            jnp.dot(picks(codes.astype(F32), rel), own_all[rel], preferred_element_type=F32), put
        )

    def put_pair(first, last, value):
        out_pair[first:last] = value.astype(BF16)

    choose(pair_ep, 1, put_pair)
    pair_across = send_of(out_pair, arrived.at[1, 1], small_sems, PAIR_ACROSS, to_pair)
    pair_across.start()

    def forward_side(step, side):
        slot = slot_of(step, side)
        got("wait_landed", landed(slot))
        to_side(0, slot, 1, across_sems, to_across).start()
        to_side(0, slot, 2, partner_sems, to_partner).start()

    def forward(step):
        for side in range(2):
            forward_side(step, side)

    if remote_lines:
        forward_side(0, 0)

    def relay(step, side):
        slot = slot_of(step, side)
        got("wait_across", to_side(1, slot, 1, across_sems, here))
        to_side(1, slot, 3, relay_sems, to_partner).start()

    got("wait_own_partner", own_copy(2, 2, 1, here))
    got("wait_own_diag", own_copy(3, 3, 2, here))
    for rel in (2, 3):
        info_copy(rel, rel, here).wait_recv()
    for rel in range(tp_size):
        info_cols[rel, :, 0:8] = turned(info[rel])
    for copy in weights[0:3]:
        copy.wait()

    def shared_expert():
        shared_rows = own_all[...].reshape(tp_size * rows_n, plan.model)
        hidden = silu(jnp.dot(shared_rows, shared_gate_w[...], preferred_element_type=F32))
        hidden = hidden * jnp.dot(shared_rows, shared_up_w[...], preferred_element_type=F32)
        shared_acc[...] = jnp.dot(
            hidden.astype(BF16), shared_down_w[...], preferred_element_type=F32
        ).reshape(shared_acc.shape)

    timed("shared", shared_expert)
    if remote_lines:
        forward_side(0, 1)

    def put_own(first, last, value, rel):
        arrived[0, rel, first:last] = value.astype(BF16)

    def choose_own():
        arrived[0, 0] = out[0]
        for rel in (1, 2, 3):
            choose(own_ep, rel, functools.partial(put_own, rel=rel))

    timed("choose_own", choose_own)

    blocks = 2 * tp_size
    tails = blocks * plan.tail
    folded = blocks * 2 * plan.block_tail

    def tail_move(side, by_column):
        shape = (folded, plan.local * tails) if by_column else (plan.local * tails, folded)
        sorted_at = iota(shape, 1 if by_column else 0)
        folded_at = iota(shape, 0 if by_column else 1)
        expert = sorted_at // tails
        block = lax.rem(sorted_at, tails) // plan.tail
        spot = lax.rem(sorted_at, plan.tail)
        target = (
            block * 2 * plan.block_tail + side * plan.block_tail + expert * plan.tail + spot
        )
        return jnp.where(folded_at == target, 1.0, 0.0).astype(BF16)

    def experts(first):
        pair = arrived.at[pl.ds(first, 2)]
        tail_rows = None
        if plan.tail:
            folded_rows = pair[:, :, 2 * bm : plan.block].reshape(folded, half)
            tail_rows = jnp.concatenate(
                [
                    jnp.dot(tail_move(side, False), folded_rows, preferred_element_type=F32)
                    for side in range(2)
                ],
                axis=1,
            ).astype(BF16)
        tail_results = []
        for expert in range(plan.local):
            pieces = []
            if plan.main:
                at = expert * plan.main
                left = pair[:, :, at : at + plan.main]
                right = pair[:, :, bm + at : bm + at + plan.main]
                pieces.append(
                    jnp.concatenate([left, right], axis=3).reshape(
                        blocks * plan.main, plan.model
                    )
                )
            if plan.tail:
                pieces.append(tail_rows[expert * tails : (expert + 1) * tails])
            x = pieces[0] if len(pieces) == 1 else jnp.concatenate(pieces, axis=0)
            hidden = silu(jnp.dot(x, gate_w[expert], preferred_element_type=F32))
            hidden = hidden * jnp.dot(x, up_w[expert], preferred_element_type=F32)
            result_rows = jnp.dot(
                hidden.astype(BF16), down_w[expert], preferred_element_type=F32
            ).astype(BF16)
            if plan.main:
                at = expert * plan.main
                shape = (2, tp_size, plan.main, half)
                count = blocks * plan.main
                part[pl.ds(first, 2), :, at : at + plan.main] = result_rows[
                    0:count, 0:half
                ].reshape(shape)
                part[pl.ds(first, 2), :, bm + at : bm + at + plan.main] = result_rows[
                    0:count, half:
                ].reshape(shape)
            if plan.tail:
                tail_results.append(result_rows[blocks * plan.main :])
        if plan.tail:
            ends = jnp.concatenate(tail_results, axis=0)
            value = jnp.dot(
                tail_move(0, True), ends[:, 0:half], preferred_element_type=F32
            ) + jnp.dot(tail_move(1, True), ends[:, half:], preferred_element_type=F32)
            part[pl.ds(first, 2), :, 2 * bm : plan.block] = value.astype(BF16).reshape(
                2, tp_size, 2 * plan.block_tail, half
            )

    def mixed(target_ep, rel, load):
        place = iota((1, plan.block), 1)
        code, side = block_code(plan, place)
        code = (code + target_ep * per_block).astype(F32)
        weight = jnp.zeros((rows_n, plan.block), F32)
        for k in range(plan.top):
            hit = code == info_cols[rel, 0:rows_n, k : k + 1]
            at = plan.top + k
            weight = weight + jnp.where(hit, info_cols[rel, 0:rows_n, at : at + 1], 0.0)
        sums = []
        for which in range(2):
            kept = jnp.where(side == which, weight, 0.0)
            high = kept.astype(BF16)
            low = (kept - high.astype(F32)).astype(BF16)
            value = jnp.dot(
                jnp.concatenate([high, low], axis=0), load(), preferred_element_type=F32
            )
            sums.append(value[0:rows_n] + value[rows_n:])
        return jnp.concatenate(sums, axis=1)

    def near(slot):
        return send_of(
            part.at[slot, pl.ds(2, 2)], near_in.at[slot], near_sems, slot, to_partner
        )

    block = arrived.at[1, 1]
    got("wait_pair_across", send_of(block, block, small_sems, PAIR_ACROSS, here))
    to_side(1, 1, 3, relay_sems, to_partner).start()
    got("wait_pair_p", to_side(2, 1, 2, partner_sems, here))
    got("wait_pair_r", to_side(3, 1, 3, relay_sems, here))
    for copy in weights[3:6]:
        copy.wait()
    timed("experts_own", experts, 0)
    near(1).start()
    if remote_lines > 1:
        forward(1)

    def fold_own():
        for rel in range(tp_size):
            shared_acc[rel] = shared_acc[rel] + mixed(own_ep, rel, lambda rel=rel: part[0, rel])

    timed("fold_own", fold_own)
    if remote_lines:
        relay(0, 0)
    shared_near[...] = shared_acc[2:4].astype(BF16)
    shared_near_copy = send_of(shared_near, near_shared, small_sems, NEAR_SHARED, to_partner)
    shared_near_copy.start()
    got("wait_near1", near(1))
    pair_out[...] = (part[1, 0:2].astype(F32) + near_in[1].astype(F32)).astype(BF16)
    pair_back = send_of(pair_out, pair_in, small_sems, PAIR_BACK, to_pair)
    pair_back.start()

    @pl.when(parity == 1)
    def attend_pair():
        block = kv_all.at[1]
        got("wait_kv_pair", send_of(block, block, kv_pair_sems, 0, here))
        timed("attend", attend_slot, 1)

    if remote_lines:
        kv_step(1)


    def ready(step):
        for side in range(2):
            slot = slot_of(step, side)
            got("wait_partner", to_side(2, slot, 2, partner_sems, here))
            got("wait_relay", to_side(3, slot, 3, relay_sems, here))

    def far(slot):
        return send_of(far_out.at[slot], far_in.at[slot], far_sems, slot, to_across)

    def twin_copy(side):
        return send_of(
            twin_out.at[side],
            twin_in.at[side],
            small_sems,
            TWIN + side,
            (from_ep(twin_from + side), own_tp),
        )

    def send_far(step):
        is_twin = (other_line(step) == twin) & outer
        for side in range(2):
            slot = slot_of(step, side)
            got("wait_near", near(slot))

            def over_x(slot=slot):
                value = part[slot, 1].astype(F32) + near_in[slot, 1].astype(F32)
                far_out[slot] = value.astype(BF16)
                far(slot).start()

            def straight(slot=slot, side=side):
                value = part[slot, 0:2].astype(F32) + near_in[slot].astype(F32)
                twin_out[side] = value.astype(BF16)
                twin_copy(side).start()

            if side in STRAIGHT:
                pl.when(is_twin)(straight)
                pl.when(jnp.logical_not(is_twin))(over_x)
            else:
                over_x()

    def give_back(slot):
        return send_of(
            total.at[slot], back.at[slot], return_sems, slot, (from_ep(slot), own_tp)
        )

    def send_total(step):
        def reduced(slot):
            got("wait_far", far(slot))
            total[slot] = (
                part[slot, 0].astype(F32)
                + near_in[slot, 0].astype(F32)
                + far_in[slot].astype(F32)
            ).astype(BF16)
            give_back(slot).start()

        for side in range(2):
            if side in STRAIGHT:
                pl.when((other_line(step) != twin) | inner)(
                    functools.partial(reduced, slot_of(step, side))
                )
            else:
                reduced(slot_of(step, side))

    def turn(step):
        @pl.when(step >= 2)
        def relay_first():
            relay(step - 1, 0)

        relay(step - 1, 1)

        @pl.when(step >= 3)
        def attend_line():
            attend_step(step - 2)

        ready(step - 1)
        timed("experts", experts, slot_of(step - 1, 0))
        for side in range(2):
            near(slot_of(step - 1, side)).start()

        send_far(step - 1)

        @pl.when(step + 1 < remote_lines)
        def next_line():
            forward(step + 1)

        @pl.when(step >= 2)
        def answer():
            send_total(step - 2)

        kv_step(step + 1)

    if remote_lines:
        each(1, remote_lines + 1, turn)

    def folded_rows(rel):
        value = shared_acc[rel] + near_shared[rel].astype(F32)
        return value + mixed(pair_ep, rel, lambda: pair_in[rel])

    def fold_twin(rel):
        value = result[...]
        for side in STRAIGHT:
            value = value + mixed(
                to_ep(twin_to + side), rel, lambda side=side: twin_in[side, rel]
            )
        result[...] = value

    got("wait_near_shared", shared_near_copy)
    got("wait_pair_back", pair_back)
    result[...] = folded_rows(1)
    if remote_lines:

        @pl.when(inner)
        def with_twin():
            for side in STRAIGHT:
                got("wait_twin", twin_copy(side))
            fold_twin(1)

    far_shared_out[...] = result[...].astype(BF16)
    shared_far_copy = send_of(far_shared_out, far_shared, small_sems, FAR_SHARED, to_across)
    shared_far_copy.start()
    each(max(remote_lines - 1, 1), remote_lines + 1, attend_step)
    weights[6].wait()
    rows_out = shard // tp_size
    mixer_term = jnp.dot(
        attended[...].astype(BF16), mixer_w[...], preferred_element_type=F32
    ).astype(BF16)
    for place in range(tp_size):
        high = lax.rem(place // 2 + own_tp // 2, 2)
        low = lax.rem(place + own_tp, 2)
        mix_part[high + 2 * low] = mixer_term[place * rows_out : (place + 1) * rows_out]
    mix_near_copy = send_of(
        mix_part.at[pl.ds(2, 2)], near_mix, small_sems, NEAR_MIX, to_partner
    )
    mix_near_copy.start()
    if remote_lines:
        send_total(remote_lines - 1)
    got("wait_near_mix", mix_near_copy)
    far_mix_out[...] = (mix_part[1].astype(F32) + near_mix[1].astype(F32)).astype(BF16)
    mix_far_copy = send_of(far_mix_out, far_mix, small_sems, FAR_MIX, to_across)
    mix_far_copy.start()
    result[...] = folded_rows(0)
    if remote_lines:
        pl.when(inner)(functools.partial(fold_twin, 0))

    rows_over_x.wait_send()
    own_copy(0, 2, 1, to_partner).wait_send()
    own_copy(1, 3, 2, to_partner).wait_send()
    for target, place in ((1, to_across), (2, to_partner), (3, to_diagonal)):
        info_copy(target, target, place).wait_send()
    go(1).wait_send()
    to_side(0, 1, 2, partner_sems, to_partner).wait_send()
    to_side(1, 1, 3, relay_sems, to_partner).wait_send()
    near(1).wait_send()
    for copy in (pair_across, pair_back, shared_near_copy, mix_near_copy):
        copy.wait_send()

    def is_straight(slot):
        found = slot < 0
        for side in STRAIGHT:
            found = found | ((slot == twin_from + side) & outer)
        return found

    def finish(slot):
        go(slot).wait_send()
        to_side(0, slot, 1, across_sems, to_across).wait_send()
        to_side(0, slot, 2, partner_sems, to_partner).wait_send()
        to_side(1, slot, 3, relay_sems, to_partner).wait_send()
        near(slot).wait_send()

        @pl.when(jnp.logical_not(is_straight(slot)))
        def reduced():
            far(slot).wait_send()

    each(2, ep_size, finish)

    if remote_lines:

        @pl.when(outer)
        def sent_twin():
            for side in STRAIGHT:
                twin_copy(side).wait_send()

    def finish_kv(step):
        @pl.when((step <= line) & (line + 1 < lines))
        def sent_on():
            kv_line(kv_all.at[2 * step], step + 1).wait_send()

        @pl.when((step <= line) & (step >= 1))
        def sent_over():
            kv_pair(kv_all.at[2 * step], step).wait_send()

    each(0, lines, finish_kv)

    @pl.when(parity == 0)
    def sent_pair():
        kv_pair(kv_ref, 0).wait_send()

    def take_back(step):
        def one(slot):
            block = back.at[slot]
            got("wait_back", send_of(block, block, return_sems, slot, here))
            result[...] = result[...] + mixed(to_ep(slot), 0, lambda: back[slot])

        for side in range(2):
            if side in STRAIGHT:
                pl.when((other_line(step) != twin) | outer)(
                    functools.partial(one, slot_to(step, side))
                )
            else:
                one(slot_to(step, side))

    each(0, remote_lines, take_back)

    def returned(slot):
        @pl.when(jnp.logical_not(is_straight(slot)))
        def one():
            give_back(slot).wait_send()

    timed("drain_returns", each, 2, ep_size, returned)
    got("wait_far_shared", shared_far_copy)
    with jax.named_scope("final_expert"):
        combined = result[...] + far_shared[...].astype(F32)
        expert_out[...] = root_norm(combined, exit_ref[...]).astype(BF16)
    expert_write = pltpu.make_async_copy(expert_out, expert_hbm_out, output_sem.at[0])
    expert_write.start()
    got("wait_far_mix", mix_far_copy)
    with jax.named_scope("final_mixer"):
        mixer_sum = mix_part[0].astype(F32) + near_mix[0].astype(F32) + far_mix[...].astype(F32)
        mixer_out[...] = root_norm(mixer_sum, mixer_gain_ref[...]).astype(BF16)
    mixer_write = pltpu.make_async_copy(mixer_out, mixer_hbm_out, output_sem.at[1])
    mixer_write.start()
    shared_far_copy.wait_send()
    mix_far_copy.wait_send()
    with jax.named_scope("writes"):
        expert_write.wait()
        mixer_write.wait()


def hand_on(mixer_in, expert_in, mixer_out, expert_out, mixer_held, expert_held, sems):
    arrays = [(expert_in, expert_held, expert_out), (mixer_in, mixer_held, mixer_out)]
    reads = [
        pltpu.make_async_copy(source, held, sems.at[0, number])
        for number, (source, held, target) in enumerate(arrays)
    ]
    writes = [
        pltpu.make_async_copy(held, target, sems.at[1, number])
        for number, (source, held, target) in enumerate(arrays)
    ]
    for read in reads:
        read.start()
    for read, write in zip(reads, writes):
        read.wait()
        write.start()
    for write in writes:
        write.wait()


def on_device(
    query_rows,
    key_rows,
    value_rows,
    key_bias,
    mixer_weight,
    mixer_gain,
    routed_input,
    entry_gain,
    expert_index,
    route_weights,
    expert_gate,
    expert_up,
    expert_down,
    shared_gate,
    shared_up,
    shared_down,
    exit_gain,
):
    ep_size = lax.axis_size("ep")
    tp_size = lax.axis_size("tp")
    plan = Plan(
        ep_size, tp_size, key_bias.shape[1], query_rows, routed_input, expert_index, expert_gate
    )
    shard, width, model, rows = plan.shard, plan.width, plan.model, plan.rows
    kv_rows = shard + -(-plan.heads // 8) * 8
    small = [
        routed_input,
        entry_gain.reshape(1, model),
        jnp.transpose(expert_index),
        jnp.transpose(route_weights),
        key_rows,
        value_rows,
        jnp.transpose(key_bias),
        query_rows,
        exit_gain.reshape(1, model),
        mixer_gain.reshape(1, model),
    ]
    large = [
        mixer_weight,
        expert_gate,
        expert_up,
        expert_down,
        shared_gate,
        shared_up,
        shared_down,
    ]
    block = (plan.block, plan.half)
    mix = (shard // tp_size, model)

    def buffer(*shape, kind=BF16):
        return pltpu.VMEM(shape, kind)

    sem = pltpu.SemaphoreType.DMA
    hbm = pl.BlockSpec(memory_space=pltpu.HBM)
    scratch = [buffer(*mix), buffer(rows, model), sem((2,))]
    scratch += [pltpu.VMEM(value.shape, value.dtype) for value in small + large]
    scratch += [
        buffer(rows, model),
        buffer(tp_size, rows, model),
        buffer(tp_size, 8, plan.padded_rows, kind=F32),
        buffer(tp_size, plan.padded_rows, 128, kind=F32),
        buffer(ep_size, *block),
        buffer(*block),
        buffer(ep_size, tp_size, *block),
        buffer(ep_size, tp_size, *block),
        buffer(ep_size, 2, *block),
        buffer(ep_size, *block),
        buffer(ep_size, *block),
        buffer(ep_size, *block),
        buffer(ep_size, *block),
        buffer(2, *block),
        buffer(2, *block),
        buffer(2, 2, *block),
        buffer(2, 2, *block),
        buffer(tp_size, rows, model, kind=F32),
        buffer(2, rows, model),
        buffer(2, rows, model),
        buffer(rows, model),
        buffer(rows, model),
        buffer(rows, model, kind=F32),
        buffer(tp_size, *mix),
        buffer(2, *mix),
        buffer(*mix),
        buffer(*mix),
        buffer(kv_rows, 2 * width),
        buffer(ep_size, kv_rows, 2 * width),
        buffer(plan.heads * shard, width),
        buffer(plan.heads * shard, shard, kind=F32),
        buffer(shard, width, kind=F32),
    ]
    scratch += [sem((len(small),)), sem((len(large),))]
    for count in (4, 4, ep_size, ep_size, ep_size, ep_size, ep_size, ep_size, ep_size, ep_size, ep_size, 8):
        scratch += [sem((count,)), sem((count,))]
    results = pl.pallas_call(
        functools.partial(layer_kernel, plan),
        out_shape=(
            jax.ShapeDtypeStruct(mix, BF16),
            jax.ShapeDtypeStruct((rows, model), BF16),
        ),
        in_specs=[hbm] * len(small + large),
        out_specs=(hbm, hbm),
        scratch_shapes=scratch,
        compiler_params=pltpu.CompilerParams(
            collective_id=0, has_side_effects=True, vmem_limit_bytes=62 * 1024 * 1024
        ),
        name="whole_layer",
    )(*small, *large)
    return pl.pallas_call(
        hand_on,
        out_shape=(
            jax.ShapeDtypeStruct(mix, BF16),
            jax.ShapeDtypeStruct((rows, model), BF16),
        ),
        in_specs=[hbm] * 2,
        out_specs=(hbm, hbm),
        scratch_shapes=[buffer(*mix), buffer(rows, model), sem((2, 2))],
        name="hand_on",
    )(*results)


def solution(mesh):
    in_specs = (
        P("ep", "tp"),
        P("ep", "tp"),
        P("ep", "tp"),
        P("ep", "tp"),
        P("tp", None),
        P(),
        P(("ep", "tp"), None),
        P(),
        P(("ep", "tp"), None),
        P(("ep", "tp"), None),
        P("ep", None, "tp"),
        P("ep", None, "tp"),
        P("ep", "tp", None),
        P(None, "tp"),
        P(None, "tp"),
        P("tp", None),
        P(),
    )
    out_specs = (P(("ep", "tp"), None), P(("ep", "tp"), None))
    return jax.shard_map(
        on_device, mesh=mesh, in_specs=in_specs, out_specs=out_specs, check_vma=False
    )
```
